256 devices in a mesh: sp: 64 (over z, x, core), tp: 4 (over y).
Axes of the slice: x: 4, y: 4, z: 8, core: 2. Of those that a mesh axis runs over, the one named last changes fastest.
Arguments:
- residual: bfloat16 [65536, 2048], P('sp'), may hold values from -6 to 6
- query: bfloat16 [65536, 1024], P('sp', 'tp'), may hold values from -6 to 6
- key: bfloat16 [65536, 256], P('sp', 'tp'), may hold values from -6 to 6
- value: bfloat16 [65536, 256], P('sp', 'tp'), may hold values from -6 to 6
- sink: float32 [16], P('tp'), may hold values from 3 to 9
- norm_gain: float32 [2048], replicated, may hold values from 0.1 to 1.9
- w_out: bfloat16 [1024, 2048], P('tp'), may hold values from -1.5 to 1.5
- w_gate: bfloat16 [2048, 4096], P('sp', 'tp'), may hold values from -0.125 to 0.125
- w_value: bfloat16 [2048, 4096], P('sp', 'tp'), may hold values from -0.125 to 0.125
- conv_gate: bfloat16 [3, 4096], P(None, 'tp'), may hold values from -3 to 3
- conv_value: bfloat16 [3, 4096], P(None, 'tp'), may hold values from -3 to 3
- w_down: bfloat16 [4096, 2048], P('tp', 'sp'), may hold values from -0.09375 to 0.09375
Outputs:
- layer_out: bfloat16 [65536, 2048], P(('sp', 'tp'))
The draws below stay inside these ranges and needn't reach their ends.
All inputs are finite; a program needn't handle non-finite values.
Results may differ from the reference program's by a relative error of at most 0.015.
Values may be sent and summed in bfloat16 or wider, within the bound.
No kernel may reach another device: no remote copies, remote signals or barrier semaphores. Data moves between devices by JAX's collectives and lax.ppermute only.
A program may use at most 128 MiB of HBM per device.

```python
import jax
import jax.numpy as jnp
from jax import lax

D = 2048
FF = 4096
HEADS = 16
KV_HEADS = 4
HD = 64
WINDOW = 128
TOKENS = 65536
N_TP = 4


def draw_key(key, part):
    base = jax.random.fold_in(key, 11)
    shape = (TOKENS, KV_HEADS * HD)
    return jnp.clip(jax.random.normal(jax.random.fold_in(base, 1), shape, jnp.float32), -6.0, 6.0).astype(jnp.bfloat16)


def draw_query(key, part):
    base = jax.random.fold_in(key, 11)
    shape = (TOKENS, HEADS * HD)
    return jnp.clip(jax.random.normal(jax.random.fold_in(base, 2), shape, jnp.float32), -6.0, 6.0).astype(jnp.bfloat16)


def steps_of(key, shape, split, smallest, top_value):
    level = 1.0
    for dim, shards_of in split:
        heights = jax.random.uniform(jax.random.fold_in(jax.random.fold_in(key, 6), dim), (shards_of,), jnp.float32, smallest / len(split), top_value / len(split))
        level = level * jnp.repeat(jnp.exp(heights), shape[dim] // shards_of).reshape((-1,) + (1,) * (len(shape) - 1 - dim))
    return level


def bell_draw(stream_key, dims, scale, most, shards=(), held_as=jnp.bfloat16):
    level = steps_of(stream_key, dims, shards, -0.22, 0.18) if shards else 1.0
    array = jax.random.normal(stream_key, dims, jnp.float32) * scale * level
    return jnp.minimum(jnp.maximum(array, -most), most).astype(held_as)


def setup_inputs(seed: int = 0) -> dict:
    key_of = jax.random.split(jax.random.key(seed), 13)
    residual = bell_draw(key_of[0], (TOKENS, D), 1.0, 6.0, ((0, 64),))
    query = draw_query(jax.random.fold_in(key_of[12], 71), 0)
    key = draw_key(jax.random.fold_in(key_of[12], 71), 0)
    value = bell_draw(key_of[3], (TOKENS, KV_HEADS * HD), 1.0, 6.0, ((0, 64), (1, 4)))
    sink = jnp.clip(3.0 + 6.0 * jax.random.uniform(key_of[4], (HEADS,), jnp.float32) ** steps_of(key_of[4], (HEADS,), ((0, 4),), -0.2, 0.2), 3.0, 9.0)
    norm_gain = jnp.clip(1.0 + 0.18 * jax.random.normal(key_of[5], (D,), jnp.float32), 0.1, 1.9)
    w_out = bell_draw(key_of[6], (HEADS * HD, D), (HD // 4) ** -0.5, 1.5, ((0, 4),))
    w_gate = bell_draw(key_of[7], (D, FF), D ** -0.5, 0.125, ((0, 64), (1, 4)))
    w_value = bell_draw(key_of[8], (D, FF), D ** -0.5, 0.125, ((0, 64), (1, 4)))
    conv_gate = bell_draw(key_of[9], (3, FF), 0.577, 3.0, ((1, 4),))
    conv_value = bell_draw(key_of[10], (3, FF), 0.577, 3.0, ((1, 4),))
    w_down = bell_draw(key_of[11], (FF, D), FF ** -0.5, 0.09375, ((0, 4), (1, 64)))
    return {"residual": residual, "query": query, "key": key, "value": value, "sink": sink, "norm_gain": norm_gain, "w_out": w_out, "w_gate": w_gate, "w_value": w_value, "conv_gate": conv_gate, "conv_value": conv_value, "w_down": w_down}


THETA = 10000.0
EPS = 1e-06

def rotate(field, positions):
    count = field.shape[0]
    parts = field.astype(jnp.float32).reshape(count, -1, HD)
    inverse = 1.0 / THETA ** (jnp.arange(0, HD, 2, dtype=jnp.float32) / HD)
    angle = positions[:, None] * inverse[None, :]
    cosine = jnp.cos(angle)[:, None, :]
    sine = jnp.sin(angle)[:, None, :]
    first = parts[..., :HD // 2]
    second = parts[..., HD // 2:]
    turned = jnp.concatenate([first * cosine - second * sine, second * cosine + first * sine], axis=-1)
    return turned.reshape(count, -1).astype(jnp.bfloat16)

def band_attention(queries, keys, values, sinks, start, total):
    count = queries.shape[0]
    blocks = count // WINDOW
    kv_local = keys.shape[1] // HD
    group = queries.shape[1] // (kv_local * HD)
    query_blocks = queries.astype(jnp.float32).reshape(blocks, WINDOW, kv_local, group, HD)
    key_band = jnp.concatenate([keys[i * WINDOW:i * WINDOW + count].reshape(blocks, WINDOW, kv_local, HD) for i in range(3)], axis=1).astype(jnp.float32)
    value_band = jnp.concatenate([values[i * WINDOW:i * WINDOW + count].reshape(blocks, WINDOW, kv_local, HD) for i in range(3)], axis=1).astype(jnp.float32)
    scores = jnp.einsum('nqkgd,njkd->nkgqj', query_blocks, key_band) * HD ** (-0.5)
    block_ids = jnp.arange(blocks, dtype=jnp.int32)[:, None]
    query_pos = start + block_ids * WINDOW + jnp.arange(WINDOW, dtype=jnp.int32)[None, :]
    key_pos = start - WINDOW + block_ids * WINDOW + jnp.arange(3 * WINDOW, dtype=jnp.int32)[None, :]
    valid = (key_pos[:, None, :] >= 0) & (key_pos[:, None, :] < total) & (jnp.abs(query_pos[:, :, None] - key_pos[:, None, :]) <= WINDOW)
    scores = jnp.where(valid[:, None, None], scores, -1e+30)
    sink_col = sinks.astype(jnp.float32).reshape(1, kv_local, group, 1, 1)
    top = jnp.maximum(lax.optimization_barrier(jnp.max(scores, axis=-1, keepdims=True)), sink_col)
    weights = jnp.exp(scores - top)
    denom = lax.optimization_barrier(jnp.sum(weights, axis=-1, keepdims=True)) + jnp.exp(sink_col - top)
    probs = (weights / denom).astype(jnp.bfloat16)
    out = jnp.einsum('nkgqj,njkd->nqkgd', probs.astype(jnp.float32), value_band)
    return out.reshape(count, kv_local * group * HD).astype(jnp.bfloat16)

def rmsnorm(field, gain):
    wide = field.astype(jnp.float32)
    scale = lax.rsqrt(lax.optimization_barrier(jnp.mean(wide * wide, axis=-1, keepdims=True)) + EPS)
    return (wide * scale * gain).astype(jnp.bfloat16)

def block_sum(left, right, pieces):
    width = left.shape[1] // pieces
    summed = jnp.zeros((left.shape[0], right.shape[1]), jnp.float32)
    for index in range(pieces):
        term = jnp.dot(left[:, index * width:(index + 1) * width], right[index * width:(index + 1) * width], preferred_element_type=jnp.float32)
        rounded = lax.optimization_barrier(term.astype(jnp.bfloat16))
        summed = summed + rounded.astype(jnp.float32)
    return summed

def reference(residual, query, key, value, sink, norm_gain, w_out, w_gate, w_value, conv_gate, conv_value, w_down):
    total = query.shape[0]
    kv_heads = key.shape[1] // HD
    group = query.shape[1] // key.shape[1]
    positions = jnp.arange(total, dtype=jnp.float32)
    turned_query = rotate(query, positions)
    turned_key = rotate(key, positions)
    pad = ((WINDOW, WINDOW), (0, 0))
    keys_ext = jnp.pad(turned_key, pad)
    values_ext = jnp.pad(value, pad)
    query_heads = turned_query.reshape(total, kv_heads, group * HD).transpose(1, 0, 2)
    key_heads = keys_ext.reshape(total + 2 * WINDOW, kv_heads, HD).transpose(1, 0, 2)
    value_heads = values_ext.reshape(total + 2 * WINDOW, kv_heads, HD).transpose(1, 0, 2)
    sink_heads = sink.reshape(kv_heads, group)

    def one_head(args):
        return band_attention(args[0], args[1], args[2], args[3], 0, total)
    outs = lax.map(one_head, (query_heads, key_heads, value_heads, sink_heads))
    attended = outs.transpose(1, 0, 2).reshape(total, -1)
    mix = block_sum(attended, w_out, N_TP)
    mid = (residual.astype(jnp.float32) + mix).astype(jnp.bfloat16)
    normed = rmsnorm(mid, norm_gain)
    gate_up = jnp.dot(normed, w_gate, preferred_element_type=jnp.float32).astype(jnp.bfloat16)
    value_up = jnp.dot(normed, w_value, preferred_element_type=jnp.float32).astype(jnp.bfloat16)

    def convolve(field, taps):
        padded = jnp.pad(field, ((1, 1), (0, 0))).astype(jnp.float32)
        taps = taps.astype(jnp.float32)
        return padded[:-2] * taps[0] + padded[1:-1] * taps[1] + padded[2:] * taps[2]
    gate_conv = convolve(gate_up, conv_gate)
    value_conv = convolve(value_up, conv_value)
    hidden = (jax.nn.silu(gate_conv) * value_conv).astype(jnp.bfloat16)
    ffn = block_sum(hidden, w_down, N_TP)
    return (mid.astype(jnp.float32) + ffn).astype(jnp.bfloat16)
```

```python
import jax
import jax.numpy as jnp
from jax import lax
from jax.experimental import pallas as pl
from jax.experimental.pallas import tpu as pltpu
from jax.sharding import PartitionSpec as P

HD = 64
WINDOW = 128
THETA = 10000.0
EPS = 1e-06
NZ, NX, NC, NY = 8, 4, 2, 4
EDGE = 16
HALO = WINDOW + EDGE
NEG = -1e30
F32 = jnp.float32
BF16 = jnp.bfloat16


def sp_index(z, x, c):
    return ((z % NZ) * NX + x % NX) * NC + c


def sp_shift(value, dz=0, dx=0, swap=False, by_core=True, flip=1):
    pairs = []
    for z in range(NZ):
        for x in range(NX):
            for c in range(NC):
                s = flip * (1 - 2 * c)
                target = sp_index(z, x, 1 - c) if swap else sp_index(z + s * dz, x + s * dx, c)
                pairs.append((sp_index(z, x, c), target))
    return lax.ppermute(value, "sp", pairs)


def tp_shift(value, flip=1, by_core=True):
    pairs = []
    for sp in range(NZ * NX * NC):
        s = flip * (1 - 2 * (sp % NC)) if by_core else flip
        for y in range(NY):
            pairs.append((sp * NY + y, sp * NY + (y + s) % NY))
    return lax.ppermute(value, ("sp", "tp"), pairs)


def half_of(value, core, rows):
    return lax.dynamic_slice_in_dim(value, core * rows, rows, 0)


def gather_gv(shard, core):
    sibling = sp_shift(shard, swap=True)
    chunk = jnp.where(
        core == 0,
        jnp.concatenate([shard, sibling], 0),
        jnp.concatenate([sibling, shard], 0),
    )
    r1 = sp_shift(chunk, dz=1)
    r2 = sp_shift(r1, dz=1)
    r3 = sp_shift(r2, dz=1)
    r4 = sp_shift(half_of(r3, core, 32), dz=1)
    h0 = jnp.concatenate([r1, r2, r3, r4, shard], 0)
    a1 = sp_shift(h0, dx=1)
    b1 = sp_shift(h0, dx=1, flip=-1)
    a2 = sp_shift(a1, dx=1)
    mine = (h0, a1, b1, a2)
    theirs = tuple(sp_shift(v, swap=True) for v in mine)
    return mine + theirs


def gather_down(shard, core):
    sibling = sp_shift(shard, swap=True)
    chunk = jnp.where(
        core == 0,
        jnp.concatenate([shard, sibling], 0),
        jnp.concatenate([sibling, shard], 0),
    )
    r1 = sp_shift(chunk, dx=1)
    r2 = sp_shift(half_of(r1, core, 32), dx=1)
    m = jnp.concatenate([shard, r1, r2], 0)
    full = jnp.concatenate([m, sp_shift(m, swap=True)], 0)
    z1 = sp_shift(full, dz=1)
    z2 = sp_shift(z1, dz=1)
    z3 = sp_shift(z2, dz=1)
    z4 = sp_shift(z3[: m.shape[0]], dz=1)
    mine = (z1, z2, z3, z4)
    theirs = tuple(sp_shift(v, swap=True) for v in mine)
    return (full,) + mine + theirs


def place_gv_kernel(pos, *refs):
    pieces, out, sems = refs[:8], refs[8], refs[9]
    z, x, c = pos[0], pos[1], pos[2]
    copies = []

    def copy(src, at, rows, dst):
        copies.append(
            pltpu.make_async_copy(
                src.at[pl.ds(at, rows)],
                out.at[pl.ds(pl.multiple_of(dst, 32), rows)],
                sems.at[len(copies)],
            )
        )

    for side in range(2):
        cc = c if side == 0 else 1 - c
        s = 1 - 2 * cc
        for index, dx in enumerate((0, -1, 1, -2)):
            src = pieces[side * 4 + index]
            base = ((x + s * dx + NX) % NX) * 64
            for k in (1, 2, 3):
                copy(src, (k - 1) * 64, 64, ((z - s * k + NZ) % NZ) * 256 + base)
            copy(src, 192, 32, ((z + 4) % NZ) * 256 + base + cc * 32)
            copy(src, 224, 32, z * 256 + base + cc * 32)
    for item in copies:
        item.start()
    for item in copies:
        item.wait()


def place_down_kernel(pos, *refs):
    pieces, out, sems = refs[:9], refs[9], refs[10]
    z, x, c = pos[0], pos[1], pos[2]
    copies = []

    def copy(src, at, rows, dst):
        copies.append(
            pltpu.make_async_copy(
                src.at[pl.ds(at, rows)],
                out.at[pl.ds(pl.multiple_of(dst, 32), rows)],
                sems.at[len(copies)],
            )
        )

    def half(src, at, zz, cc):
        s = 1 - 2 * cc
        base = ((zz + NZ) % NZ) * 256
        copy(src, at, 32, base + x * 64 + cc * 32)
        copy(src, at + 32, 64, base + ((x - s + NX) % NX) * 64)
        copy(src, at + 96, 32, base + ((x + 2) % NX) * 64 + cc * 32)

    half(pieces[0], 0, z, c)
    half(pieces[0], 128, z, 1 - c)
    for side in range(2):
        cc = c if side == 0 else 1 - c
        s = 1 - 2 * cc
        for k in (1, 2, 3):
            src = pieces[1 + side * 4 + k - 1]
            half(src, 0, z - s * k, cc)
            half(src, 128, z - s * k, 1 - cc)
        half(pieces[1 + side * 4 + 3], 0, z + 4, cc)
    for item in copies:
        item.start()
    for item in copies:
        item.wait()


def place(kernel, pos, pieces, shape, count):
    any_spec = pl.BlockSpec(memory_space=pl.ANY)
    return pl.pallas_call(
        kernel,
        in_specs=[pl.BlockSpec(memory_space=pltpu.SMEM)] + [any_spec] * len(pieces),
        out_specs=pl.BlockSpec(memory_space=pltpu.VMEM),
        out_shape=jax.ShapeDtypeStruct(shape, BF16),
        scratch_shapes=[pltpu.SemaphoreType.DMA((count,))],
        cost_estimate=pl.CostEstimate(
            flops=20_000_000, bytes_accessed=4 * shape[0] * shape[1], transcendentals=0
        ),
        name="place",
    )(pos, *pieces)


def attention_kernel(start_ref, sink_ref, q_ref, edge_ref, kv_ref, cos_ref, sin_ref, out_ref,
                     cos_s, sin_s, kr_s, vx_s, *, total):
    step = pl.program_id(0)
    start = start_ref[0]
    rows_kv = kv_ref.shape[0]
    packed = rows_kv // 4

    @pl.when(step == 0)
    def _():
        lane_p = lax.broadcasted_iota(jnp.int32, (packed, 128), 1)

        def spread(table, part):
            one = jnp.where(lane_p // 32 == part, table, 0.0)
            one = one + pltpu.roll(one, 32, 1)
            return one + pltpu.roll(one, 64, 1)

        sign = jnp.where(lane_p % 64 < 32, -1.0, 1.0)
        cos_p, sin_p = cos_ref[...], sin_ref[...]
        for part in range(4):
            cos_s[part * packed:(part + 1) * packed] = spread(cos_p, part)
            sin_s[part * packed:(part + 1) * packed] = spread(sin_p, part) * sign
        kv = kv_ref[...].astype(F32)
        lane = lax.broadcasted_iota(jnp.int32, (rows_kv, 128), 1)
        swapped = jnp.where(lane % 64 < 32, pltpu.roll(kv, 96, 1), pltpu.roll(kv, 32, 1))
        turned = kv * cos_s[...] + swapped * sin_s[...]
        kr_s[...] = jnp.where(lane < 64, turned, 0.0).astype(BF16)
        vx_s[...] = jnp.where(lane < 64, pltpu.roll(kv, 64, 1), 1.0).astype(BF16)

    def attend(q, at, window, first, out_at):
        rows = q.shape[0]
        span = 3 * WINDOW
        lane = lax.broadcasted_iota(jnp.int32, (rows, 128), 1)
        cos = cos_s[pl.ds(at, rows)]
        sin = sin_s[pl.ds(at, rows)]
        stack = []
        for pair in range(2):
            part = q[:, pair * 128:(pair + 1) * 128].astype(F32)
            swapped = jnp.where(lane % 64 < 32, pltpu.roll(part, 96, 1), pltpu.roll(part, 32, 1))
            turned = (part * cos + swapped * sin).astype(BF16).astype(F32) * HD ** (-0.5)
            stack.append(jnp.where(lane < 64, turned, 0.0).astype(BF16))
            stack.append(jnp.where(lane < 64, pltpu.roll(turned, 64, 1), 0.0).astype(BF16))
        stacked = jnp.concatenate(stack, axis=0)
        keys = kr_s[pl.ds(window, span)]
        values = vx_s[pl.ds(window, span)]
        scores = lax.dot_general(
            stacked, keys, (((1,), (1,)), ((), ())), preferred_element_type=F32
        )
        row_pos = first + lax.broadcasted_iota(jnp.int32, (rows, span), 0)
        col_pos = (start - HALO + window) + lax.broadcasted_iota(jnp.int32, (rows, span), 1)
        apart = row_pos - col_pos
        valid = (apart <= WINDOW) & (apart >= -WINDOW) & (col_pos >= 0) & (col_pos < total)
        weights, sink_terms = [], []
        for head in range(4):
            mine = jnp.where(valid, scores[head * rows:(head + 1) * rows], NEG)
            sink = sink_ref[head]
            top = jnp.maximum(jnp.max(mine, axis=1, keepdims=True), sink)
            weights.append(jnp.exp(mine - top).astype(BF16))
            sink_terms.append(jnp.exp(sink - top))
        both = jnp.dot(jnp.concatenate(weights, axis=0), values, preferred_element_type=F32)
        heads = []
        for head in range(4):
            mine = both[head * rows:(head + 1) * rows]
            heads.append(mine / (pltpu.roll(mine, 64, 1) + sink_terms[head]))
        for pair in range(2):
            joined = jnp.where(lane < 64, heads[2 * pair], pltpu.roll(heads[2 * pair + 1], 64, 1))
            out_ref[pl.ds(out_at, rows), pair * 128:(pair + 1) * 128] = joined.astype(BF16)

    base = pl.multiple_of(step * WINDOW, WINDOW)
    attend(q_ref[...], base + HALO, base + EDGE, start + base, base)

    @pl.when(step == pl.num_programs(0) - 1)
    def _():
        count = out_ref.shape[0] - 2 * EDGE
        attend(edge_ref[0:EDGE], HALO - EDGE, 0, start - EDGE, count)
        attend(
            edge_ref[EDGE:2 * EDGE], HALO + count, rows_kv - 3 * WINDOW, start + count, count + EDGE
        )


def attention(start, sink, query, edges, kv, cos, sin, total):
    count = query.shape[0]
    rows_kv = kv.shape[0]
    blocks = count // WINDOW
    whole = lambda shape: pl.BlockSpec(shape, lambda i: (0, 0))
    smem = pl.BlockSpec(memory_space=pltpu.SMEM)
    import functools

    return pl.pallas_call(
        functools.partial(attention_kernel, total=total),
        grid=(blocks,),
        in_specs=[
            smem,
            smem,
            pl.BlockSpec((WINDOW, 256), lambda i: (i, 0)),
            whole(edges.shape),
            whole(kv.shape),
            whole(cos.shape),
            whole(sin.shape),
        ],
        out_specs=whole((count + 2 * EDGE, 256)),
        out_shape=jax.ShapeDtypeStruct((count + 2 * EDGE, 256), BF16),
        scratch_shapes=[
            pltpu.VMEM((rows_kv, 128), F32),
            pltpu.VMEM((rows_kv, 128), F32),
            pltpu.VMEM((rows_kv, 128), BF16),
            pltpu.VMEM((rows_kv, 128), BF16),
        ],
        compiler_params=pltpu.CompilerParams(dimension_semantics=("arbitrary",)),
        cost_estimate=pl.CostEstimate(
            flops=1_600_000_000, bytes_accessed=3_000_000, transcendentals=1_700_000
        ),
        name="attention",
    )(start, sink, query, edges, kv, cos, sin)


def mix_kernel(info, own, left, right, far, w_own, w_left, w_right, w_mine, w_other,
               res, res_edge, gain, mid_ref, norm_ref, edge_ref, w_far):
    step = pl.program_id(0)
    core, start, total = info[0], info[1], info[2]
    rows = res.shape[0]
    count = own.shape[0] - 2 * EDGE

    @pl.when(step == 0)
    def _():
        w_far[pl.ds(pl.multiple_of(core * 128, 128), 128)] = w_mine[...]
        w_far[pl.ds(pl.multiple_of((1 - core) * 128, 128), 128)] = w_other[...]

    main = pl.multiple_of(step * rows, rows)
    edge = pl.multiple_of(count + step * EDGE, EDGE)

    def block(ref):
        return jnp.concatenate([ref[pl.ds(main, rows)], ref[pl.ds(edge, EDGE)]], axis=0)

    acc = jnp.dot(block(own), w_own[...], preferred_element_type=F32)
    acc = acc + jnp.dot(block(left), w_left[...], preferred_element_type=F32)
    acc = acc + jnp.dot(block(right), w_right[...], preferred_element_type=F32)
    acc = acc + jnp.dot(block(far), w_far[...], preferred_element_type=F32)
    resid = jnp.concatenate([res[...], res_edge[...]], axis=0).astype(F32)
    mid = (resid + acc).astype(BF16)
    wide = mid.astype(F32)
    scale = lax.rsqrt(jnp.mean(wide * wide, axis=1, keepdims=True) + EPS)
    normed = wide * scale * gain[...]
    mid_ref[...] = mid[:rows]
    norm_ref[...] = normed[:rows].astype(BF16)
    at = jnp.where(step == 0, start - EDGE, start + count)
    pos = at + lax.broadcasted_iota(jnp.int32, (EDGE, 1), 0)
    inside = (pos >= 0) & (pos < total)
    edge_ref[...] = jnp.where(inside, normed[rows:], 0.0).astype(BF16)


def mix(info, parts, weights, residual, res_edges, gain):
    count, width = residual.shape
    steps = 2
    rows = count // steps
    whole = lambda a: pl.BlockSpec(a.shape, lambda i: (0, 0))
    return pl.pallas_call(
        mix_kernel,
        grid=(steps,),
        in_specs=[pl.BlockSpec(memory_space=pltpu.SMEM)]
        + [whole(a) for a in parts]
        + [whole(a) for a in weights]
        + [
            pl.BlockSpec((rows, width), lambda i: (i, 0)),
            pl.BlockSpec((EDGE, width), lambda i: (i, 0)),
            whole(gain),
        ],
        out_specs=[
            pl.BlockSpec((rows, width), lambda i: (i, 0)),
            pl.BlockSpec((rows, width), lambda i: (i, 0)),
            pl.BlockSpec((EDGE, width), lambda i: (i, 0)),
        ],
        out_shape=[
            jax.ShapeDtypeStruct((count, width), BF16),
            jax.ShapeDtypeStruct((count, width), BF16),
            jax.ShapeDtypeStruct((2 * EDGE, width), BF16),
        ],
        scratch_shapes=[pltpu.VMEM((256, width), BF16)],
        compiler_params=pltpu.CompilerParams(dimension_semantics=("arbitrary",)),
        cost_estimate=pl.CostEstimate(
            flops=2 * 1056 * 1024 * 2048, bytes_accessed=20_000_000, transcendentals=1056
        ),
        name="mix",
    )(info, *parts, *weights, residual, res_edges, gain)


def ffn_kernel(info, norm_ref, edge_ref, wg, wv, wd, taps_g, taps_v, *rest, add_at):
    if add_at is None:
        out_ref, xs, acc, sems = rest
        add_ref = None
    else:
        add_ref, out_ref, xs, acc, sems = rest
    step = pl.program_id(0)
    quarter = info[0]
    last = norm_ref.shape[0] // 256 - 1
    at = pl.multiple_of(quarter * 256, 256)

    @pl.when(step == 0)
    def _():
        copy = pltpu.make_async_copy(norm_ref.at[pl.ds(at, 256)], xs.at[pl.ds(EDGE, 256)], sems.at[0])
        copy.start()

        @pl.when(quarter == 0)
        def _():
            pltpu.sync_copy(edge_ref.at[pl.ds(0, EDGE)], xs.at[pl.ds(0, EDGE)])

        @pl.when(quarter != 0)
        def _():
            before = pl.multiple_of(jnp.maximum(at - EDGE, 0), EDGE)
            pltpu.sync_copy(norm_ref.at[pl.ds(before, EDGE)], xs.at[pl.ds(0, EDGE)])

        @pl.when(quarter == last)
        def _():
            pltpu.sync_copy(edge_ref.at[pl.ds(EDGE, EDGE)], xs.at[pl.ds(256 + EDGE, EDGE)])

        @pl.when(quarter != last)
        def _():
            after = pl.multiple_of(jnp.minimum(at + 256, last * 256), EDGE)
            pltpu.sync_copy(norm_ref.at[pl.ds(after, EDGE)], xs.at[pl.ds(256 + EDGE, EDGE)])

        copy.wait()

    rows = 256 + 2 * EDGE

    def convolve(weight, taps):
        up = jnp.dot(xs[...], weight[...], preferred_element_type=F32).astype(BF16).astype(F32)
        out = (
            pltpu.roll(up, 1, 0) * taps[0:1]
            + up * taps[1:2]
            + pltpu.roll(up, rows - 1, 0) * taps[2:3]
        )
        return out[EDGE:EDGE + 256]

    gate = convolve(wg, taps_g[...])
    value = convolve(wv, taps_v[...])
    hidden = (gate / (1.0 + jnp.exp(-gate)) * value).astype(BF16)
    term = lax.dot_general(hidden, wd[...], (((1,), (1,)), ((), ())), preferred_element_type=F32)

    @pl.when(step == 0)
    def _():
        acc[...] = term

    @pl.when(step != 0)
    def _():
        acc[...] += term

    @pl.when(step == pl.num_programs(0) - 1)
    def _():
        if add_at is None:
            out_ref[...] = acc[...].astype(out_ref.dtype)
        else:
            other = 128 - add_at
            out_ref[add_at:add_at + 128] = (
                acc[add_at:add_at + 128] + add_ref[...].astype(F32)
            ).astype(out_ref.dtype)
            out_ref[other:other + 128] = acc[other:other + 128].astype(out_ref.dtype)


def ffn(info, normed, edges, w_up, w_down, taps_g, taps_v, addend=None, add_at=None, dtype=BF16):
    import functools

    width = normed.shape[1]
    hidden = w_down.shape[1]
    block = 256
    steps = hidden // block
    any_spec = pl.BlockSpec(memory_space=pl.ANY)
    in_specs = [
        pl.BlockSpec(memory_space=pltpu.SMEM),
        any_spec,
        any_spec,
        pl.BlockSpec((width, block), lambda i: (0, i)),
        pl.BlockSpec((width, block), lambda i: (0, i + steps)),
        pl.BlockSpec((width, block), lambda i: (0, i)),
        pl.BlockSpec((8, block), lambda i: (0, i)),
        pl.BlockSpec((8, block), lambda i: (0, i)),
    ]
    operands = [info, normed, edges, w_up, w_up, w_down, taps_g, taps_v]
    if addend is not None:
        in_specs.append(pl.BlockSpec(addend.shape, lambda i: (0, 0)))
        operands.append(addend)
    return pl.pallas_call(
        functools.partial(ffn_kernel, add_at=add_at),
        grid=(steps,),
        in_specs=in_specs,
        out_specs=pl.BlockSpec((256, width), lambda i: (0, 0)),
        out_shape=jax.ShapeDtypeStruct((256, width), dtype),
        scratch_shapes=[
            pltpu.VMEM((256 + 2 * EDGE, width), BF16),
            pltpu.VMEM((256, width), F32),
            pltpu.SemaphoreType.DMA((1,)),
        ],
        compiler_params=pltpu.CompilerParams(dimension_semantics=("arbitrary",)),
        cost_estimate=pl.CostEstimate(
            flops=2 * 256 * 2048 * 3072, bytes_accessed=15_000_000, transcendentals=262144
        ),
        name="ffn",
    )(*operands)


def shards(
    residual, query, key, value, sink, norm_gain, w_out, w_gate, w_value, conv_gate, conv_value,
    w_down,
):
    count, width = residual.shape
    sp = lax.axis_index("sp")
    tp = lax.axis_index("tp")
    start = sp * count
    total = count * lax.axis_size("sp")
    core = sp % NC
    place_at = jnp.stack([sp // (NX * NC), (sp // NC) % NX, core]).astype(jnp.int32)

    gv_pieces = gather_gv(jnp.concatenate([w_gate, w_value], axis=1), core)
    down_pieces = gather_down(w_down.T, core)

    kv = jnp.concatenate([key, value], axis=1)

    def packed(rows, at):
        return jnp.concatenate(
            [
                rows,
                query[at:at + 1].reshape(2, 128),
                residual[at:at + 1].reshape(16, 128),
                jnp.zeros((14, 128), BF16),
            ],
            axis=0,
        )

    n_sp = lax.axis_size("sp")
    forward = [(i, i + 1) for i in range(n_sp - 1)]
    backward = [(i + 1, i) for i in range(n_sp - 1)]
    low = lax.ppermute(packed(kv[-HALO:], count - 1), "sp", forward)
    high = lax.ppermute(packed(kv[:HALO], 0), "sp", backward)
    kv_ext = jnp.concatenate([low[:HALO], kv, high[:HALO]], axis=0)

    def edges(width_128):
        at = HALO if width_128 == 2 else HALO + 2
        cols = width_128 * 128
        pad = jnp.zeros((EDGE - 1, cols), BF16)
        return jnp.concatenate(
            [
                pad,
                low[at:at + width_128].reshape(1, cols),
                high[at:at + width_128].reshape(1, cols),
                pad,
            ],
            axis=0,
        )

    q_edges = edges(2)
    res_edges = edges(16)

    wo_left = tp_shift(w_out)
    wo_mine = tp_shift(half_of(wo_left, core, 128))
    wo_right = sp_shift(wo_left, swap=True)
    wo_other = sp_shift(wo_mine, swap=True)

    rows_kv = count + 2 * HALO
    inverse = 1.0 / THETA ** (jnp.arange(0, HD, 2, dtype=F32) / HD)
    quarter_rows = rows_kv // 4
    lane = jnp.arange(128, dtype=jnp.int32)
    position = (
        (start - HALO)
        + jnp.arange(quarter_rows, dtype=jnp.int32)[:, None]
        + (lane // 32)[None, :] * quarter_rows
    ).astype(F32)
    angle = position * jnp.tile(inverse, 4)[None, :]

    start_ref = jnp.reshape(start, (1,)).astype(jnp.int32)
    mine = attention(
        start_ref, sink, query, q_edges, kv_ext, jnp.cos(angle), jnp.sin(angle), total
    )

    left = tp_shift(mine)
    right = tp_shift(mine, flip=-1)
    rows_half = mine.shape[0] // 2
    far = jnp.concatenate(
        [tp_shift(left[:rows_half]), tp_shift(right[rows_half:], flip=-1)], axis=0
    )

    info = jnp.stack([core, start, jnp.int32(total)]).astype(jnp.int32)
    mid, normed, norm_edges = mix(
        info,
        (mine, left, right, far),
        (w_out, wo_left, wo_right, wo_mine, wo_other),
        residual,
        res_edges,
        norm_gain.reshape(1, width),
    )

    w_up = place(place_gv_kernel, place_at, gv_pieces, (width, 2 * w_gate.shape[1]), 40)
    w_dn = place(place_down_kernel, place_at, down_pieces, (width, w_gate.shape[1]), 48)

    pad8 = lambda taps: jnp.pad(taps.astype(F32), ((0, 5), (0, 0)))
    taps_g, taps_v = pad8(conv_gate), pad8(conv_value)

    def quarter(shift, addend=None, add_at=None, dtype=BF16):
        index = jnp.reshape((tp + shift) % NY, (1,)).astype(jnp.int32)
        return ffn(index, normed, norm_edges, w_up, w_dn, taps_g, taps_v, addend, add_at, dtype)

    opposite = quarter(2)
    from_low = tp_shift(opposite[:128], flip=1, by_core=False)
    from_high = tp_shift(opposite[128:], flip=-1, by_core=False)
    up = quarter(1, from_low, 0)
    got_up = tp_shift(up, flip=1, by_core=False)
    down = quarter(3, from_high, 128)
    got_down = tp_shift(down, flip=-1, by_core=False)
    own = quarter(0, dtype=F32)
    mid_rows = lax.dynamic_slice_in_dim(mid, tp * 256, 256, 0)
    out = mid_rows.astype(F32) + own + got_up.astype(F32) + got_down.astype(F32)
    return out.astype(BF16)


def solution(mesh):
    return jax.shard_map(
        shards,
        mesh=mesh,
        in_specs=(
            P("sp", None),
            P("sp", "tp"),
            P("sp", "tp"),
            P("sp", "tp"),
            P("tp"),
            P(),
            P("tp", None),
            P("sp", "tp"),
            P("sp", "tp"),
            P(None, "tp"),
            P(None, "tp"),
            P("tp", "sp"),
        ),
        out_specs=P(("sp", "tp"), None),
        check_vma=False,
    )
```

```python
import functools

import jax
import jax.numpy as jnp
from jax import lax
from jax.experimental import pallas as pl
from jax.experimental.pallas import tpu as pltpu
from jax.sharding import PartitionSpec as P


HD = 64
WINDOW = 128
THETA = 10000.0
EPS = 1e-06
NZ, NX, NC, NY = 8, 4, 2, 4
EDGE = 16
HALO = WINDOW + EDGE
NEG = -1e30
F32 = jnp.float32
BF16 = jnp.bfloat16


def sp_index(z, x, c):
    return ((z % NZ) * NX + x % NX) * NC + c


def sp_shift(value, dz=0, dx=0, swap=False, flip=1):
    pairs = []
    for z in range(NZ):
        for x in range(NX):
            for c in range(NC):
                s = flip * (1 - 2 * c)
                target = sp_index(z, x, 1 - c) if swap else sp_index(z + s * dz, x + s * dx, c)
                pairs.append((sp_index(z, x, c), target))
    return lax.ppermute(value, "sp", pairs)


def tp_shift(value, flip=1, by_core=True):
    pairs = []
    for sp in range(NZ * NX * NC):
        s = flip * (1 - 2 * (sp % NC)) if by_core else flip
        for y in range(NY):
            pairs.append((sp * NY + y, sp * NY + (y + s) % NY))
    return lax.ppermute(value, ("sp", "tp"), pairs)


def in_vmem(value):
    return pltpu.with_memory_space_constraint(value, pltpu.VMEM)


def half_of(value, core, rows):
    return lax.dynamic_slice_in_dim(value, core * rows, rows, 0)


def joined(core, shard, sibling):
    return jnp.where(
        core == 0,
        jnp.concatenate([shard, sibling], 0),
        jnp.concatenate([sibling, shard], 0),
    )


def gather_gv_rows(shard, core):
    chunk = joined(core, shard, sp_shift(shard, swap=True))
    r1 = sp_shift(chunk, dz=1)
    r2 = sp_shift(r1, dz=1)
    r3 = sp_shift(r2, dz=1)
    return chunk, r1, r2, r3


def gather_gv(shard, core, r1, r2, r3):
    r4 = sp_shift(half_of(r3, core, 32), dz=1)
    h0 = jnp.concatenate([r1, r2, r3, r4, shard], 0)
    a1 = sp_shift(h0, dx=1)
    b1 = sp_shift(h0, dx=1, flip=-1)
    a2 = sp_shift(a1, dx=1)
    mine = (h0, a1, b1, a2)
    theirs = tuple(sp_shift(v, swap=True) for v in mine)
    return mine, theirs


def gather_down(shard, core, place_at, late):
    chunk = joined(core, shard, sp_shift(shard, swap=True))
    r1 = sp_shift(chunk, dx=1)
    r1, _ = lax.optimization_barrier((r1, late))
    r2 = sp_shift(half_of(r1, core, 32), dx=1)
    m = jnp.concatenate([shard, r1, r2], 0)
    other = sp_shift(m, swap=True)
    full = place(place_x_kernel, place_at, (m, other), (256, shard.shape[1]), 6)
    z1 = sp_shift(full, dz=1)
    z2 = sp_shift(z1, dz=1)
    z3 = sp_shift(z2, dz=1)
    half = place(place_half_kernel, place_at, (z3,), (128, shard.shape[1]), 1)
    z4 = sp_shift(half, dz=1)
    mine = (z1, z2, z3, z4)
    theirs = tuple(sp_shift(v, swap=True) for v in mine)
    return (full,) + mine + theirs


def copier(out, sems):
    copies = []

    def copy(src, at, rows, dst):
        copies.append(
            pltpu.make_async_copy(
                src.at[pl.ds(at, rows)],
                out.at[pl.ds(pl.multiple_of(dst, 32), rows)],
                sems.at[len(copies)],
            )
        )

    return copies, copy


def copies_of_set(copy, src, zxc, dx, other):
    z, x, c = zxc
    cc = 1 - c if other else c
    s = 1 - 2 * cc
    base = ((x + s * dx + NX) % NX) * 64
    for k in (1, 2, 3):
        copy(src, (k - 1) * 64, 64, ((z - s * k + NZ) % NZ) * 256 + base)
    copy(src, 192, 32, ((z + 4) % NZ) * 256 + base + cc * 32)
    copy(src, 224, 32, z * 256 + base + cc * 32)


def run_copies(copies):
    for item in copies:
        item.start()
    for item in copies:
        item.wait()


def place_rest_kernel(pos, *refs, offsets):
    count = 2 * len(offsets)
    pieces, out, sems = refs[:count], refs[count + 1], refs[count + 2]
    copies, copy = copier(out, sems)
    for index, dx in enumerate(offsets):
        for other in (False, True):
            src = pieces[2 * index + other]
            copies_of_set(copy, src, (pos[0], pos[1], pos[2]), dx, other)
    run_copies(copies)


def place_x_kernel(pos, mine, theirs, out, sems):
    x, c = pos[1], pos[2]
    copies, copy = copier(out, sems)
    for src, cc in ((mine, c), (theirs, 1 - c)):
        s = 1 - 2 * cc
        copy(src, 0, 32, x * 64 + cc * 32)
        copy(src, 32, 64, ((x - s + NX) % NX) * 64)
        copy(src, 96, 32, ((x + 2) % NX) * 64 + cc * 32)
    run_copies(copies)


def place_half_kernel(pos, src, out, sems):
    at = pl.multiple_of(pos[2] * 128, 128)
    copy = pltpu.make_async_copy(src.at[pl.ds(at, 128)], out, sems.at[0])
    copy.start()
    copy.wait()


def place_down_kernel(pos, *refs):
    pieces, out, sems = refs[:9], refs[9], refs[10]
    z, c = pos[0], pos[2]
    copies, copy = copier(out, sems)
    copy(pieces[0], 0, 256, z * 256)
    for side in range(2):
        cc = c if side == 0 else 1 - c
        s = 1 - 2 * cc
        for k in (1, 2, 3):
            copy(pieces[side * 4 + k], 0, 256, ((z - s * k + NZ) % NZ) * 256)
        copy(pieces[side * 4 + 4], 0, 128, ((z + 4) % NZ) * 256 + cc * 128)
    run_copies(copies)


def place_rest(pos, pieces, offsets, w_up):
    any_spec = pl.BlockSpec(memory_space=pl.ANY)
    vmem = pl.BlockSpec(memory_space=pltpu.VMEM)
    count = len(pieces)
    return pl.pallas_call(
        functools.partial(place_rest_kernel, offsets=offsets),
        in_specs=[pl.BlockSpec(memory_space=pltpu.SMEM)] + [any_spec] * count + [vmem],
        out_specs=vmem,
        out_shape=pltpu.VMEM(w_up.shape, BF16),
        input_output_aliases={count + 1: 0},
        scratch_shapes=[pltpu.SemaphoreType.DMA((5 * count,))],
        compiler_params=pltpu.CompilerParams(vmem_limit_bytes=2 << 20),
        cost_estimate=pl.CostEstimate(
            flops=20_000_000, bytes_accessed=2_000_000 * count, transcendentals=0
        ),
    )(pos, *pieces, in_vmem(w_up))


def place(kernel, pos, pieces, shape, count):
    any_spec = pl.BlockSpec(memory_space=pl.ANY)
    return pl.pallas_call(
        kernel,
        in_specs=[pl.BlockSpec(memory_space=pltpu.SMEM)] + [any_spec] * len(pieces),
        out_specs=pl.BlockSpec(memory_space=pltpu.VMEM),
        out_shape=pltpu.VMEM(shape, BF16),
        scratch_shapes=[pltpu.SemaphoreType.DMA((count,))],
        compiler_params=pltpu.CompilerParams(vmem_limit_bytes=2 << 20),
        cost_estimate=pl.CostEstimate(
            flops=20_000_000, bytes_accessed=4 * shape[0] * shape[1], transcendentals=0
        ),
    )(pos, *pieces)


def attention_kernel(start_ref, sink_ref, q_ref, edge_ref, kv_ref, cos_ref, sin_ref, out_ref,
                     cos_s, sin_s, kr_s, vx_s, *, total):
    step = pl.program_id(0)
    start = start_ref[0]
    rows_kv = kv_ref.shape[0]
    packed = rows_kv // 4

    @pl.when(step == 0)
    def _():
        lane_p = lax.broadcasted_iota(jnp.int32, (packed, 128), 1)

        def spread(table, part):
            one = jnp.where(lane_p // 32 == part, table, 0.0)
            one = one + pltpu.roll(one, 32, 1)
            return one + pltpu.roll(one, 64, 1)

        sign = jnp.where(lane_p % 64 < 32, -1.0, 1.0)
        cos_p, sin_p = cos_ref[...], sin_ref[...]
        for part in range(4):
            cos_s[part * packed:(part + 1) * packed] = spread(cos_p, part)
            sin_s[part * packed:(part + 1) * packed] = spread(sin_p, part) * sign
        kv = kv_ref[...].astype(F32)
        lane = lax.broadcasted_iota(jnp.int32, (rows_kv, 128), 1)
        swapped = jnp.where(lane % 64 < 32, pltpu.roll(kv, 96, 1), pltpu.roll(kv, 32, 1))
        turned = kv * cos_s[...] + swapped * sin_s[...]
        kr_s[...] = jnp.where(lane < 64, turned, 0.0).astype(BF16)
        vx_s[...] = jnp.where(lane < 64, pltpu.roll(kv, 64, 1), 1.0).astype(BF16)

    def attend(q, at, window, first, out_at):
        rows = q.shape[0]
        span = 3 * WINDOW
        lane = lax.broadcasted_iota(jnp.int32, (rows, 128), 1)
        cos = cos_s[pl.ds(at, rows)]
        sin = sin_s[pl.ds(at, rows)]
        stack = []
        for pair in range(2):
            part = q[:, pair * 128:(pair + 1) * 128].astype(F32)
            swapped = jnp.where(lane % 64 < 32, pltpu.roll(part, 96, 1), pltpu.roll(part, 32, 1))
            turned = (part * cos + swapped * sin).astype(BF16).astype(F32) * HD ** (-0.5)
            stack.append(jnp.where(lane < 64, turned, 0.0).astype(BF16))
            stack.append(jnp.where(lane < 64, pltpu.roll(turned, 64, 1), 0.0).astype(BF16))
        stacked = jnp.concatenate(stack, axis=0)
        keys = kr_s[pl.ds(window, span)]
        values = vx_s[pl.ds(window, span)]
        scores = lax.dot_general(
            stacked, keys, (((1,), (1,)), ((), ())), preferred_element_type=F32
        )
        row_pos = first + lax.broadcasted_iota(jnp.int32, (rows, span), 0)
        col_pos = (start - HALO + window) + lax.broadcasted_iota(jnp.int32, (rows, span), 1)
        apart = row_pos - col_pos
        valid = (apart <= WINDOW) & (apart >= -WINDOW) & (col_pos >= 0) & (col_pos < total)
        weights, sink_terms = [], []
        for head in range(4):
            mine = jnp.where(valid, scores[head * rows:(head + 1) * rows], NEG)
            sink = sink_ref[head]
            top = jnp.maximum(jnp.max(mine, axis=1, keepdims=True), sink)
            weights.append(jnp.exp(mine - top).astype(BF16))
            sink_terms.append(jnp.exp(sink - top))
        both = jnp.dot(jnp.concatenate(weights, axis=0), values, preferred_element_type=F32)
        heads = []
        for head in range(4):
            mine = both[head * rows:(head + 1) * rows]
            heads.append(mine / (pltpu.roll(mine, 64, 1) + sink_terms[head]))
        for pair in range(2):
            joined = jnp.where(lane < 64, heads[2 * pair], pltpu.roll(heads[2 * pair + 1], 64, 1))
            out_ref[pl.ds(out_at, rows), pair * 128:(pair + 1) * 128] = joined.astype(BF16)

    base = pl.multiple_of(step * WINDOW, WINDOW)
    attend(q_ref[...], base + HALO, base + EDGE, start + base, base)

    @pl.when(step == pl.num_programs(0) - 1)
    def _():
        count = out_ref.shape[0] - 2 * EDGE

        @pl.loop(0, 2)
        def _(side):
            at = pl.multiple_of(side * EDGE, EDGE)
            attend(
                edge_ref[pl.ds(at, EDGE)],
                pl.multiple_of(HALO - EDGE + side * (count + EDGE), EDGE),
                pl.multiple_of(side * (rows_kv - 3 * WINDOW), EDGE),
                start - EDGE + side * (count + EDGE),
                pl.multiple_of(count + at, EDGE),
            )


def attention(start, sink, query, edges, kv, cos, sin, total):
    count = query.shape[0]
    rows_kv = kv.shape[0]
    blocks = count // WINDOW
    whole = lambda shape: pl.BlockSpec(shape, lambda i: (0, 0))
    smem = pl.BlockSpec(memory_space=pltpu.SMEM)
    return pl.pallas_call(
        functools.partial(attention_kernel, total=total),
        grid=(blocks,),
        in_specs=[
            smem,
            smem,
            pl.BlockSpec((WINDOW, 256), lambda i: (i, 0)),
            whole(edges.shape),
            whole(kv.shape),
            whole(cos.shape),
            whole(sin.shape),
        ],
        out_specs=whole((count + 2 * EDGE, 256)),
        out_shape=jax.ShapeDtypeStruct((count + 2 * EDGE, 256), BF16),
        scratch_shapes=[
            pltpu.VMEM((rows_kv, 128), F32),
            pltpu.VMEM((rows_kv, 128), F32),
            pltpu.VMEM((rows_kv, 128), BF16),
            pltpu.VMEM((rows_kv, 128), BF16),
        ],
        compiler_params=pltpu.CompilerParams(
            dimension_semantics=("arbitrary",), vmem_limit_bytes=16 << 20
        ),
        cost_estimate=pl.CostEstimate(
            flops=1_600_000_000, bytes_accessed=3_000_000, transcendentals=1_700_000
        ),
        name="attention",
    )(start, sink, query, edges, kv, cos, sin)


def mix_kernel(info, own, left, right, far_a, far_b, w_own, w_left, w_right, w_mine, w_other,
               res, res_edge, gain, h0, h0t, norm_ref, mid_ref, up_ref,
               far, w_far, acc, sems):
    core, start, total, tp = info[0], info[1], info[2], info[3]
    zxc = (info[4], info[5], core)
    copies, copy = copier(up_ref, sems)
    copies_of_set(copy, h0, zxc, 0, False)
    copies_of_set(copy, h0t, zxc, 0, True)
    for item in copies:
        item.start()
    count = res.shape[0]
    far[:far_a.shape[0]] = far_a[...]
    far[far_a.shape[0]:] = far_b[...]
    w_far[pl.ds(pl.multiple_of(core * 128, 128), 128)] = w_mine[...]
    w_far[pl.ds(pl.multiple_of((1 - core) * 128, 128), 128)] = w_other[...]

    width = res.shape[1]
    step = 1024

    def project(at, rows, resid, out):
        @pl.loop(0, width // step)
        def _(index):
            cols = pl.ds(pl.multiple_of(index * step, step), step)
            term = resid(cols).astype(F32)
            for ref, weight in ((own, w_own), (left, w_left), (right, w_right), (far, w_far)):
                term = term + jnp.dot(
                    ref[pl.ds(at, rows)], weight[:, cols], preferred_element_type=F32
                )
            out[:rows, cols] = term

    def norm(total):
        mid = total.astype(BF16)
        wide = mid.astype(F32)
        scale = lax.rsqrt(jnp.mean(wide * wide, axis=1, keepdims=True) + EPS)
        return mid, wide * scale * gain[...]

    @pl.loop(0, count // 256)
    def _(part):
        at = pl.multiple_of(part * 256, 256)
        project(at, 256, lambda cols: res[pl.ds(at, 256), cols], acc)

        mid, normed = norm(acc[...])
        norm_ref[pl.ds(pl.multiple_of(EDGE + at, EDGE), 256)] = normed.astype(BF16)

        @pl.when(tp == part)
        def _():
            mid_ref[...] = mid

    project(count, 2 * EDGE, lambda cols: res_edge[:, cols], acc)
    _, normed = norm(acc[:2 * EDGE])
    index = lax.broadcasted_iota(jnp.int32, (2 * EDGE, 1), 0)
    pos = start - EDGE + index + jnp.where(index < EDGE, 0, count)
    inside = (pos >= 0) & (pos < total)
    normed = jnp.where(inside, normed, 0.0).astype(BF16)
    norm_ref[0:EDGE] = normed[:EDGE]
    norm_ref[EDGE + count:2 * EDGE + count] = normed[EDGE:]
    for item in copies:
        item.wait()


def mix(info, parts, weights, residual, res_edges, gain, pieces, up_shape):
    count, width = residual.shape
    vmem = pl.BlockSpec(memory_space=pltpu.VMEM)
    any_spec = pl.BlockSpec(memory_space=pl.ANY)
    operands = [in_vmem(a) for a in (*parts, *weights, residual)] + [res_edges, gain]
    return pl.pallas_call(
        mix_kernel,
        in_specs=[pl.BlockSpec(memory_space=pltpu.SMEM)] + [vmem] * len(operands)
        + [any_spec] * len(pieces),
        out_specs=[vmem, vmem, vmem],
        out_shape=[
            pltpu.VMEM((count + 2 * EDGE, width), BF16),
            pltpu.VMEM((256, width), BF16),
            pltpu.VMEM(up_shape, BF16),
        ],
        scratch_shapes=[
            pltpu.VMEM((count + 2 * EDGE, 256), BF16),
            pltpu.VMEM((256, width), BF16),
            pltpu.VMEM((256, width), F32),
            pltpu.SemaphoreType.DMA((10,)),
        ],
        compiler_params=pltpu.CompilerParams(vmem_limit_bytes=20 << 20),
        cost_estimate=pl.CostEstimate(
            flops=2 * 1056 * 1024 * 2048, bytes_accessed=20_000_000, transcendentals=1056
        ),
        name="mix",
    )(info, *operands, *pieces)


def ffn_kernel(info, x, w_up, w_dn, taps_g, taps_v, *rest):
    rest, acc = rest[:-1], rest[-1]
    rows = 256 + 2 * EDGE
    hidden_all = w_dn.shape[1]
    block = 256

    @pl.loop(0, info.shape[0])
    def _(turn):
        at = pl.multiple_of(info[turn] * 256, 256)

        def convolve(first, taps):
            up = jnp.dot(
                x[pl.ds(at, rows)], w_up[:, pl.ds(first, block)], preferred_element_type=F32
            )
            up = up.astype(BF16).astype(F32)
            out = (
                pltpu.roll(up, 1, 0) * taps[0:1]
                + up * taps[1:2]
                + pltpu.roll(up, rows - 1, 0) * taps[2:3]
            )
            return out[EDGE:EDGE + 256]

        if rest[0].shape[0] == 256:
            acc[...] = rest[0][...].astype(F32)
        else:
            acc[...] = jnp.zeros(acc.shape, F32)

        @pl.loop(0, hidden_all // block)
        def _(step):
            first = pl.multiple_of(step * block, block)
            gate = convolve(first, taps_g[:, pl.ds(first, block)])
            value = convolve(
                pl.multiple_of(hidden_all + first, block), taps_v[:, pl.ds(first, block)]
            )
            hidden = (gate / (1.0 + jnp.exp(-gate)) * value).astype(BF16)
            acc[...] += lax.dot_general(
                hidden, w_dn[:, pl.ds(first, block)], (((1,), (1,)), ((), ())),
                preferred_element_type=F32,
            )

        outs = rest[-1:] if rest[-1].shape[0] == 256 else rest
        for index in range(len(outs) // 2):
            @pl.when(turn == index)
            def _():
                outs[2 * index][...] = acc[:128].astype(outs[2 * index].dtype)
                outs[2 * index + 1][...] = acc[128:].astype(outs[2 * index + 1].dtype)
        if len(outs) == 1:
            outs[0][...] = acc[...]


def ffn(info, normed, w_up, w_down, taps_g, taps_v, dtypes=None, mid=None):
    width = normed.shape[1]
    vmem = pl.BlockSpec(memory_space=pltpu.VMEM)
    operands = [in_vmem(normed), in_vmem(w_up), in_vmem(w_down), taps_g, taps_v]
    if mid is None:
        out_shape = [pltpu.VMEM((128, width), d) for d in dtypes]
        out_specs = [vmem] * len(dtypes)
    else:
        operands.append(in_vmem(mid))
        out_shape, out_specs = pltpu.VMEM((256, width), F32), vmem
    return pl.pallas_call(
        ffn_kernel,
        in_specs=[pl.BlockSpec(memory_space=pltpu.SMEM)] + [vmem] * len(operands),
        out_specs=out_specs,
        out_shape=out_shape,
        scratch_shapes=[pltpu.VMEM((256, width), F32)],
        compiler_params=pltpu.CompilerParams(vmem_limit_bytes=20 << 20),
        cost_estimate=pl.CostEstimate(
            flops=2 * 256 * 2048 * 3072 * info.shape[0], bytes_accessed=15_000_000, transcendentals=262144
        ),
    )(info, *operands)


def add_kernel(one, other, out):
    out[...] = (one[...] + other[...].astype(F32)).astype(BF16)


def add_rows(one, other):
    vmem = pl.BlockSpec(memory_space=pltpu.VMEM)
    return pl.pallas_call(
        add_kernel,
        in_specs=[vmem, vmem],
        out_specs=vmem,
        out_shape=pltpu.VMEM(one.shape, BF16),
        compiler_params=pltpu.CompilerParams(vmem_limit_bytes=2 << 20),
        cost_estimate=pl.CostEstimate(flops=300_000, bytes_accessed=2_000_000, transcendentals=0),
        name="add_rows",
    )(in_vmem(one), in_vmem(other))


def final_kernel(own, up_a, up_b, down_a, down_b, out):
    for part, ups, downs in ((0, up_a, down_a), (128, up_b, down_b)):
        out[part:part + 128] = (
            own[part:part + 128] + ups[...].astype(F32) + downs[...].astype(F32)
        ).astype(BF16)


def final_sum(*operands):
    vmem = pl.BlockSpec(memory_space=pltpu.VMEM)
    return pl.pallas_call(
        final_kernel,
        in_specs=[vmem] * len(operands),
        out_specs=vmem,
        out_shape=jax.ShapeDtypeStruct(operands[0].shape, BF16),
        compiler_params=pltpu.CompilerParams(vmem_limit_bytes=8 << 20),
        cost_estimate=pl.CostEstimate(
            flops=2_000_000, bytes_accessed=5_000_000, transcendentals=0
        ),
        name="final",
    )(*(in_vmem(a) for a in operands))


def layer(
    residual, query, key, value, sink, norm_gain, w_out, w_gate, w_value, conv_gate, conv_value,
    w_down,
):
    count, width = residual.shape
    sp = lax.axis_index("sp")
    tp = lax.axis_index("tp")
    start = sp * count
    total = count * lax.axis_size("sp")
    core = sp % NC
    place_at = jnp.stack([sp // (NX * NC), (sp // NC) % NX, core]).astype(jnp.int32)

    gv_shard = jnp.concatenate([w_gate, w_value], axis=1)
    chunk, gv_1, late, gv_3 = gather_gv_rows(gv_shard, core)
    gv_2 = late
    chunk, key, value, query, residual_edge = lax.optimization_barrier(
        (chunk, key, value, query, (residual[:1], residual[count - 1:]))
    )
    down_pieces = gather_down(w_down.T, core, place_at, late)

    kv = jnp.concatenate([key, value], axis=1)

    def packed(rows, at, resid):
        return jnp.concatenate(
            [
                rows,
                query[at:at + 1].reshape(2, 128),
                resid.reshape(16, 128),
                jnp.zeros((14, 128), BF16),
            ],
            axis=0,
        )

    n_sp = lax.axis_size("sp")
    forward = [(i, i + 1) for i in range(n_sp - 1)]
    backward = [(i + 1, i) for i in range(n_sp - 1)]
    low = lax.ppermute(packed(kv[-HALO:], count - 1, residual_edge[1]), "sp", forward)
    high = lax.ppermute(packed(kv[:HALO], 0, residual_edge[0]), "sp", backward)
    low, high, _ = lax.optimization_barrier((low, high, late))
    kv_ext = jnp.concatenate([low[:HALO], kv, high[:HALO]], axis=0)

    def edges(width_128):
        at = HALO if width_128 == 2 else HALO + 2
        cols = width_128 * 128
        pad = jnp.zeros((EDGE - 1, cols), BF16)
        return jnp.concatenate(
            [
                pad,
                low[at:at + width_128].reshape(1, cols),
                high[at:at + width_128].reshape(1, cols),
                pad,
            ],
            axis=0,
        )

    q_edges = edges(2)
    res_edges = edges(16)

    wo_left = tp_shift(w_out)
    wo_mine = tp_shift(half_of(wo_left, core, 128))
    wo_right = sp_shift(wo_left, swap=True)
    wo_other = sp_shift(wo_mine, swap=True)

    rows_kv = count + 2 * HALO
    inverse = 1.0 / THETA ** (jnp.arange(0, HD, 2, dtype=F32) / HD)
    quarter_rows = rows_kv // 4
    lane = jnp.arange(128, dtype=jnp.int32)
    position = (
        (start - HALO)
        + jnp.arange(quarter_rows, dtype=jnp.int32)[:, None]
        + (lane // 32)[None, :] * quarter_rows
    ).astype(F32)
    angle = position * jnp.tile(inverse, 4)[None, :]

    start_ref = jnp.reshape(start, (1,)).astype(jnp.int32)
    mine = attention(start_ref, sink, query, q_edges, kv_ext, jnp.cos(angle), jnp.sin(angle), total)

    info = jnp.stack(
        [core, start, jnp.int32(total), tp, place_at[0], place_at[1]]
    ).astype(jnp.int32)
    pad8 = lambda taps: jnp.pad(taps.astype(F32), ((0, 5), (0, 0)))
    indices = tuple(
        jnp.stack([(tp + shift) % NY for shift in turns]).astype(jnp.int32)
        for turns in ((0,), (2,), (1, 3))
    )
    mine, info, place_late, taps_g, taps_v, indices, res_edges, gain = lax.optimization_barrier(
        (mine, info, place_at, pad8(conv_gate), pad8(conv_value), indices, res_edges,
         norm_gain.reshape(1, width))
    )

    gv_3, mine = lax.optimization_barrier((gv_3, mine))
    gv_mine, gv_theirs = gather_gv(gv_shard, core, gv_1, gv_2, gv_3)

    left = tp_shift(mine)
    right = tp_shift(mine, flip=-1)
    far_a = tp_shift(left[:512])
    far_b = tp_shift(right[512:], flip=-1)

    normed, mid, w_up = mix(
        info,
        (mine, left, right, far_a, far_b),
        (w_out, wo_left, wo_right, wo_mine, wo_other),
        residual,
        res_edges,
        gain,
        gv_mine[:1] + gv_theirs[:1],
        (width, 2 * w_gate.shape[1]),
    )

    w_dn = place(place_down_kernel, place_late, down_pieces, (width, w_gate.shape[1]), 9)
    sets = (gv_mine[1], gv_theirs[1], gv_mine[2], gv_theirs[2])
    w_up = place_rest(place_late, sets, (-1, 1), w_up)
    w_up = place_rest(place_late, (gv_mine[3], gv_theirs[3]), (-2,), w_up)

    def quarter(index, **kwargs):
        return ffn(index, normed, w_up, w_dn, taps_g, taps_v, **kwargs)

    opp_a, opp_b = quarter(indices[1], dtypes=(BF16, BF16))
    from_low = tp_shift(opp_a, flip=1, by_core=False)
    from_high = tp_shift(opp_b, flip=-1, by_core=False)
    up_a, up_b, down_a, down_b = quarter(indices[2], dtypes=(F32, BF16, BF16, F32))
    got_up_b = tp_shift(up_b, flip=1, by_core=False)
    got_down_a = tp_shift(down_a, flip=-1, by_core=False)
    up_a = add_rows(up_a, from_low)
    got_up_a = tp_shift(up_a, flip=1, by_core=False)
    down_b = add_rows(down_b, from_high)
    got_down_b = tp_shift(down_b, flip=-1, by_core=False)
    own = quarter(indices[0], mid=mid)
    return final_sum(own, got_up_a, got_up_b, got_down_a, got_down_b)


def solution(mesh):
    return jax.shard_map(
        layer,
        mesh=mesh,
        in_specs=(
            P("sp", None),
            P("sp", "tp"),
            P("sp", "tp"),
            P("sp", "tp"),
            P("tp"),
            P(),
            P("tp", None),
            P("sp", "tp"),
            P("sp", "tp"),
            P(None, "tp"),
            P(None, "tp"),
            P("tp", "sp"),
        ),
        out_specs=P(("sp", "tp"), None),
        check_vma=False,
    )
```

```python
import functools

import jax
import jax.numpy as jnp
from jax import lax
from jax.experimental import pallas as pl
from jax.experimental.pallas import tpu as pltpu
from jax.sharding import PartitionSpec as P


HD = 64
WINDOW = 128
THETA = 10000.0
EPS = 1e-06
NZ, NX, NC, NY = 8, 4, 2, 4
EDGE = 16
HALO = WINDOW + EDGE
NEG = -1e30
F32 = jnp.float32
BF16 = jnp.bfloat16


def sp_index(z, x, c):
    return ((z % NZ) * NX + x % NX) * NC + c


def sp_shift(value, dz=0, dx=0, swap=False, flip=1):
    pairs = []
    for z in range(NZ):
        for x in range(NX):
            for c in range(NC):
                s = flip * (1 - 2 * c)
                target = sp_index(z, x, 1 - c) if swap else sp_index(z + s * dz, x + s * dx, c)
                pairs.append((sp_index(z, x, c), target))
    return lax.ppermute(value, "sp", pairs)


def tp_shift(value, flip=1, by_core=True):
    pairs = []
    for sp in range(NZ * NX * NC):
        s = flip * (1 - 2 * (sp % NC)) if by_core else flip
        for y in range(NY):
            pairs.append((sp * NY + y, sp * NY + (y + s) % NY))
    return lax.ppermute(value, ("sp", "tp"), pairs)


def in_vmem(value):
    return pltpu.with_memory_space_constraint(value, pltpu.VMEM)


def half_of(value, core, rows):
    return lax.dynamic_slice_in_dim(value, core * rows, rows, 0)


def joined(core, shard, sibling):
    return jnp.where(
        core == 0,
        jnp.concatenate([shard, sibling], 0),
        jnp.concatenate([sibling, shard], 0),
    )


def gather_gv_rows(shard, core):
    chunk = joined(core, shard, sp_shift(shard, swap=True))
    r1 = sp_shift(chunk, dz=1)
    r2 = sp_shift(r1, dz=1)
    r3 = sp_shift(r2, dz=1)
    return chunk, r1, r2, r3


def gather_gv(shard, core, r1, r2, r3):
    r4 = sp_shift(half_of(r3, core, 32), dz=1)
    h0 = jnp.concatenate([r1, r2, r3, r4, shard], 0)
    a1 = sp_shift(h0, dx=1)
    b1 = sp_shift(h0, dx=1, flip=-1)
    a2 = sp_shift(a1, dx=1)
    mine = (h0, a1, b1, a2)
    theirs = tuple(sp_shift(v, swap=True) for v in mine)
    return mine, theirs


def gather_down(shard, core, place_at, late):
    chunk = joined(core, shard, sp_shift(shard, swap=True))
    r1 = sp_shift(chunk, dx=1)
    r1, _ = lax.optimization_barrier((r1, late))
    r2 = sp_shift(half_of(r1, core, 32), dx=1)
    m = jnp.concatenate([shard, r1, r2], 0)
    other = sp_shift(m, swap=True)
    full = place(place_x_kernel, place_at, (m, other), (256, shard.shape[1]), 6)
    z1 = sp_shift(full, dz=1)
    z2 = sp_shift(z1, dz=1)
    z3 = sp_shift(z2, dz=1)
    half = place(place_half_kernel, place_at, (z3,), (128, shard.shape[1]), 1)
    z4 = sp_shift(half, dz=1)
    mine = (z1, z2, z3, z4)
    theirs = tuple(sp_shift(v, swap=True) for v in mine)
    return (full,) + mine + theirs


def copier(out, sems):
    copies = []

    def copy(src, at, rows, dst):
        copies.append(
            pltpu.make_async_copy(
                src.at[pl.ds(at, rows)],
                out.at[pl.ds(pl.multiple_of(dst, 32), rows)],
                sems.at[len(copies)],
            )
        )

    return copies, copy


def copies_of_set(copy, src, zxc, dx, other):
    z, x, c = zxc
    cc = 1 - c if other else c
    s = 1 - 2 * cc
    base = ((x + s * dx + NX) % NX) * 64
    for k in (1, 2, 3):
        copy(src, (k - 1) * 64, 64, ((z - s * k + NZ) % NZ) * 256 + base)
    copy(src, 192, 32, ((z + 4) % NZ) * 256 + base + cc * 32)
    copy(src, 224, 32, z * 256 + base + cc * 32)


def run_copies(copies):
    for item in copies:
        item.start()
    for item in copies:
        item.wait()


def place_rest_kernel(pos, *refs, offsets):
    count = 2 * len(offsets)
    pieces, out, sems = refs[:count], refs[count + 1], refs[count + 2]
    copies, copy = copier(out, sems)
    for index, dx in enumerate(offsets):
        for other in (False, True):
            src = pieces[2 * index + other]
            copies_of_set(copy, src, (pos[0], pos[1], pos[2]), dx, other)
    run_copies(copies)


def place_x_kernel(pos, mine, theirs, out, sems):
    x, c = pos[1], pos[2]
    copies, copy = copier(out, sems)
    for src, cc in ((mine, c), (theirs, 1 - c)):
        s = 1 - 2 * cc
        copy(src, 0, 32, x * 64 + cc * 32)
        copy(src, 32, 64, ((x - s + NX) % NX) * 64)
        copy(src, 96, 32, ((x + 2) % NX) * 64 + cc * 32)
    run_copies(copies)


def place_half_kernel(pos, src, out, sems):
    at = pl.multiple_of(pos[2] * 128, 128)
    copy = pltpu.make_async_copy(src.at[pl.ds(at, 128)], out, sems.at[0])
    copy.start()
    copy.wait()


def place_down_kernel(pos, *refs):
    pieces, out, sems = refs[:9], refs[9], refs[10]
    z, c = pos[0], pos[2]
    copies, copy = copier(out, sems)
    copy(pieces[0], 0, 256, z * 256)
    for side in range(2):
        cc = c if side == 0 else 1 - c
        s = 1 - 2 * cc
        for k in (1, 2, 3):
            copy(pieces[side * 4 + k], 0, 256, ((z - s * k + NZ) % NZ) * 256)
        copy(pieces[side * 4 + 4], 0, 128, ((z + 4) % NZ) * 256 + cc * 128)
    run_copies(copies)


def place_rest(pos, pieces, offsets, w_up):
    any_spec = pl.BlockSpec(memory_space=pl.ANY)
    vmem = pl.BlockSpec(memory_space=pltpu.VMEM)
    count = len(pieces)
    return pl.pallas_call(
        functools.partial(place_rest_kernel, offsets=offsets),
        in_specs=[pl.BlockSpec(memory_space=pltpu.SMEM)] + [any_spec] * count + [vmem],
        out_specs=vmem,
        out_shape=pltpu.VMEM(w_up.shape, BF16),
        input_output_aliases={count + 1: 0},
        scratch_shapes=[pltpu.SemaphoreType.DMA((5 * count,))],
        compiler_params=pltpu.CompilerParams(vmem_limit_bytes=2 << 20),
        cost_estimate=pl.CostEstimate(
            flops=20_000_000, bytes_accessed=2_000_000 * count, transcendentals=0
        ),
    )(pos, *pieces, in_vmem(w_up))


def place(kernel, pos, pieces, shape, count):
    any_spec = pl.BlockSpec(memory_space=pl.ANY)
    return pl.pallas_call(
        kernel,
        in_specs=[pl.BlockSpec(memory_space=pltpu.SMEM)] + [any_spec] * len(pieces),
        out_specs=pl.BlockSpec(memory_space=pltpu.VMEM),
        out_shape=pltpu.VMEM(shape, BF16),
        scratch_shapes=[pltpu.SemaphoreType.DMA((count,))],
        compiler_params=pltpu.CompilerParams(vmem_limit_bytes=2 << 20),
        cost_estimate=pl.CostEstimate(
            flops=20_000_000, bytes_accessed=4 * shape[0] * shape[1], transcendentals=0
        ),
    )(pos, *pieces)


def attention_kernel(start_ref, sink_ref, q_ref, edge_ref, kv_ref, cos_ref, sin_ref, out_ref,
                     cos_s, sin_s, kr_s, vx_s, *, total):
    step = pl.program_id(0)
    start = start_ref[0]
    rows_kv = kv_ref.shape[0]
    packed = rows_kv // 4

    @pl.when(step == 0)
    def _():
        lane_p = lax.broadcasted_iota(jnp.int32, (packed, 128), 1)

        def spread(table, part):
            one = jnp.where(lane_p // 32 == part, table, 0.0)
            one = one + pltpu.roll(one, 32, 1)
            return one + pltpu.roll(one, 64, 1)

        sign = jnp.where(lane_p % 64 < 32, -1.0, 1.0)
        cos_p, sin_p = cos_ref[...], sin_ref[...]
        for part in range(4):
            cos_s[part * packed:(part + 1) * packed] = spread(cos_p, part)
            sin_s[part * packed:(part + 1) * packed] = spread(sin_p, part) * sign
        kv = kv_ref[...].astype(F32)
        lane = lax.broadcasted_iota(jnp.int32, (rows_kv, 128), 1)
        swapped = jnp.where(lane % 64 < 32, pltpu.roll(kv, 96, 1), pltpu.roll(kv, 32, 1))
        turned = kv * cos_s[...] + swapped * sin_s[...]
        kr_s[...] = jnp.where(lane < 64, turned, 0.0).astype(BF16)
        vx_s[...] = jnp.where(lane < 64, pltpu.roll(kv, 64, 1), 1.0).astype(BF16)

    def attend(q, at, window, first, out_at):
        rows = q.shape[0]
        span = 3 * WINDOW
        lane = lax.broadcasted_iota(jnp.int32, (rows, 128), 1)
        cos = cos_s[pl.ds(at, rows)]
        sin = sin_s[pl.ds(at, rows)]
        stack = []
        for pair in range(2):
            part = q[:, pair * 128:(pair + 1) * 128].astype(F32)
            swapped = jnp.where(lane % 64 < 32, pltpu.roll(part, 96, 1), pltpu.roll(part, 32, 1))
            turned = (part * cos + swapped * sin).astype(BF16).astype(F32) * HD ** (-0.5)
            stack.append(jnp.where(lane < 64, turned, 0.0).astype(BF16))
            stack.append(jnp.where(lane < 64, pltpu.roll(turned, 64, 1), 0.0).astype(BF16))
        stacked = jnp.concatenate(stack, axis=0)
        keys = kr_s[pl.ds(window, span)]
        values = vx_s[pl.ds(window, span)]
        scores = lax.dot_general(
            stacked, keys, (((1,), (1,)), ((), ())), preferred_element_type=F32
        )
        row_pos = first + lax.broadcasted_iota(jnp.int32, (rows, span), 0)
        col_pos = (start - HALO + window) + lax.broadcasted_iota(jnp.int32, (rows, span), 1)
        apart = row_pos - col_pos
        valid = (apart <= WINDOW) & (apart >= -WINDOW) & (col_pos >= 0) & (col_pos < total)
        weights, sink_terms = [], []
        for head in range(4):
            mine = jnp.where(valid, scores[head * rows:(head + 1) * rows], NEG)
            sink = sink_ref[head]
            top = jnp.maximum(jnp.max(mine, axis=1, keepdims=True), sink)
            weights.append(jnp.exp(mine - top).astype(BF16))
            sink_terms.append(jnp.exp(sink - top))
        both = jnp.dot(jnp.concatenate(weights, axis=0), values, preferred_element_type=F32)
        heads = []
        for head in range(4):
            mine = both[head * rows:(head + 1) * rows]
            heads.append(mine / (pltpu.roll(mine, 64, 1) + sink_terms[head]))
        for pair in range(2):
            joined = jnp.where(lane < 64, heads[2 * pair], pltpu.roll(heads[2 * pair + 1], 64, 1))
            out_ref[pl.ds(out_at, rows), pair * 128:(pair + 1) * 128] = joined.astype(BF16)

    base = pl.multiple_of(step * WINDOW, WINDOW)
    attend(q_ref[...], base + HALO, base + EDGE, start + base, base)

    @pl.when(step == pl.num_programs(0) - 1)
    def _():
        count = out_ref.shape[0] - 2 * EDGE

        @pl.loop(0, 2)
        def _(side):
            at = pl.multiple_of(side * EDGE, EDGE)
            attend(
                edge_ref[pl.ds(at, EDGE)],
                pl.multiple_of(HALO - EDGE + side * (count + EDGE), EDGE),
                pl.multiple_of(side * (rows_kv - 3 * WINDOW), EDGE),
                start - EDGE + side * (count + EDGE),
                pl.multiple_of(count + at, EDGE),
            )


def attention(start, sink, query, edges, kv, cos, sin, total):
    count = query.shape[0]
    rows_kv = kv.shape[0]
    blocks = count // WINDOW
    whole = lambda shape: pl.BlockSpec(shape, lambda i: (0, 0))
    smem = pl.BlockSpec(memory_space=pltpu.SMEM)
    return pl.pallas_call(
        functools.partial(attention_kernel, total=total),
        grid=(blocks,),
        in_specs=[
            smem,
            smem,
            pl.BlockSpec((WINDOW, 256), lambda i: (i, 0)),
            whole(edges.shape),
            whole(kv.shape),
            whole(cos.shape),
            whole(sin.shape),
        ],
        out_specs=whole((count + 2 * EDGE, 256)),
        out_shape=jax.ShapeDtypeStruct((count + 2 * EDGE, 256), BF16),
        scratch_shapes=[
            pltpu.VMEM((rows_kv, 128), F32),
            pltpu.VMEM((rows_kv, 128), F32),
            pltpu.VMEM((rows_kv, 128), BF16),
            pltpu.VMEM((rows_kv, 128), BF16),
        ],
        compiler_params=pltpu.CompilerParams(
            dimension_semantics=("arbitrary",), vmem_limit_bytes=16 << 20
        ),
        cost_estimate=pl.CostEstimate(
            flops=1_600_000_000, bytes_accessed=3_000_000, transcendentals=1_700_000
        ),
        name="attention",
    )(start, sink, query, edges, kv, cos, sin)


def mix_kernel(info, own, left, right, far_a, far_b, w_own, w_left, w_right, w_mine, w_other,
               res, res_edge, gain, h0, h0t, norm_ref, mid_ref, up_ref,
               far, w_far, acc, sems):
    core, start, total, tp = info[0], info[1], info[2], info[3]
    zxc = (info[4], info[5], core)
    copies, copy = copier(up_ref, sems)
    copies_of_set(copy, h0, zxc, 0, False)
    copies_of_set(copy, h0t, zxc, 0, True)
    for item in copies:
        item.start()
    count = res.shape[0]
    far[:far_a.shape[0]] = far_a[...]
    far[far_a.shape[0]:] = far_b[...]
    w_far[pl.ds(pl.multiple_of(core * 128, 128), 128)] = w_mine[...]
    w_far[pl.ds(pl.multiple_of((1 - core) * 128, 128), 128)] = w_other[...]

    width = res.shape[1]
    step = 512

    def project(at, rows, resid, out):
        @pl.loop(0, width // step)
        def _(index):
            cols = pl.ds(pl.multiple_of(index * step, step), step)
            term = resid(cols).astype(F32)
            for ref, weight in ((own, w_own), (left, w_left), (right, w_right), (far, w_far)):
                term = term + jnp.dot(
                    ref[pl.ds(at, rows)], weight[:, cols], preferred_element_type=F32
                )
            out[:rows, cols] = term

    def norm(total):
        mid = total.astype(BF16)
        wide = mid.astype(F32)
        scale = lax.rsqrt(jnp.mean(wide * wide, axis=1, keepdims=True) + EPS)
        return mid, wide * scale * gain[...]

    @pl.loop(0, count // 256)
    def _(part):
        at = pl.multiple_of(part * 256, 256)
        project(at, 256, lambda cols: res[pl.ds(at, 256), cols], acc)

        @pl.loop(0, 4)
        def _(group):
            rows = pl.multiple_of(group * 64, 64)
            mid, normed = norm(acc[pl.ds(rows, 64)])
            norm_ref[pl.ds(pl.multiple_of(EDGE + at + rows, EDGE), 64)] = normed.astype(BF16)

            @pl.when(tp == part)
            def _():
                mid_ref[pl.ds(rows, 64)] = mid

    project(count, 2 * EDGE, lambda cols: res_edge[:, cols], acc)
    _, normed = norm(acc[:2 * EDGE])
    index = lax.broadcasted_iota(jnp.int32, (2 * EDGE, 1), 0)
    pos = start - EDGE + index + jnp.where(index < EDGE, 0, count)
    inside = (pos >= 0) & (pos < total)
    normed = jnp.where(inside, normed, 0.0).astype(BF16)
    norm_ref[0:EDGE] = normed[:EDGE]
    norm_ref[EDGE + count:2 * EDGE + count] = normed[EDGE:]
    for item in copies:
        item.wait()


def mix(info, parts, weights, residual, res_edges, gain, pieces, up_shape):
    count, width = residual.shape
    vmem = pl.BlockSpec(memory_space=pltpu.VMEM)
    any_spec = pl.BlockSpec(memory_space=pl.ANY)
    operands = [in_vmem(a) for a in (*parts, *weights, residual)] + [res_edges, gain]
    return pl.pallas_call(
        mix_kernel,
        in_specs=[pl.BlockSpec(memory_space=pltpu.SMEM)] + [vmem] * len(operands)
        + [any_spec] * len(pieces),
        out_specs=[vmem, vmem, vmem],
        out_shape=[
            pltpu.VMEM((count + 2 * EDGE, width), BF16),
            pltpu.VMEM((256, width), BF16),
            pltpu.VMEM(up_shape, BF16),
        ],
        scratch_shapes=[
            pltpu.VMEM((count + 2 * EDGE, 256), BF16),
            pltpu.VMEM((256, width), BF16),
            pltpu.VMEM((256, width), F32),
            pltpu.SemaphoreType.DMA((10,)),
        ],
        compiler_params=pltpu.CompilerParams(vmem_limit_bytes=20 << 20),
        cost_estimate=pl.CostEstimate(
            flops=2 * 1056 * 1024 * 2048, bytes_accessed=20_000_000, transcendentals=1056
        ),
        name="mix",
    )(info, *operands, *pieces)


def ffn_kernel(info, x, w_up, w_dn, taps_all, *rest):
    rest, acc, conv = rest[:-2], rest[-2], rest[-1]
    rows = 256 + 2 * EDGE
    hidden_all = w_dn.shape[1]
    block = 256

    @pl.loop(0, info.shape[0])
    def _(turn):
        at = pl.multiple_of(info[turn] * 256, 256)

        def convolve(first, taps):
            up = jnp.dot(
                x[pl.ds(at, rows)], w_up[:, pl.ds(first, block)], preferred_element_type=F32
            )
            up = up.astype(BF16).astype(F32)
            out = (
                pltpu.roll(up, 1, 0) * taps[0:1]
                + up * taps[1:2]
                + pltpu.roll(up, rows - 1, 0) * taps[2:3]
            )
            return out[EDGE:EDGE + 256]

        if rest[0].shape[0] == 256:
            acc[...] = rest[0][...].astype(F32)
        else:
            acc[...] = jnp.zeros(acc.shape, F32)

        @pl.loop(0, hidden_all // block)
        def _(step):
            first = pl.multiple_of(step * block, block)

            @pl.loop(0, 2)
            def _(side):
                cols = pl.multiple_of(side * hidden_all + first, block)
                conv[pl.ds(pl.multiple_of(side * 256, 256), 256)] = convolve(
                    cols, taps_all[:, pl.ds(cols, block)]
                )

            gate, value = conv[:256], conv[256:]
            hidden = (gate / (1.0 + jnp.exp(-gate)) * value).astype(BF16)
            acc[...] += lax.dot_general(
                hidden, w_dn[:, pl.ds(first, block)], (((1,), (1,)), ((), ())),
                preferred_element_type=F32,
            )

        outs = rest[-1:] if rest[-1].shape[0] == 256 else rest
        for index in range(len(outs) // 2):
            @pl.when(turn == index)
            def _():
                outs[2 * index][...] = acc[:128].astype(outs[2 * index].dtype)
                outs[2 * index + 1][...] = acc[128:].astype(outs[2 * index + 1].dtype)
        if len(outs) == 1:
            outs[0][...] = acc[...]


def ffn(info, normed, w_up, w_down, taps, dtypes=None, mid=None):
    width = normed.shape[1]
    vmem = pl.BlockSpec(memory_space=pltpu.VMEM)
    operands = [in_vmem(normed), in_vmem(w_up), in_vmem(w_down), taps]
    if mid is None:
        out_shape = [pltpu.VMEM((128, width), d) for d in dtypes]
        out_specs = [vmem] * len(dtypes)
    else:
        operands.append(in_vmem(mid))
        out_shape, out_specs = pltpu.VMEM((256, width), F32), vmem
    return pl.pallas_call(
        ffn_kernel,
        in_specs=[pl.BlockSpec(memory_space=pltpu.SMEM)] + [vmem] * len(operands),
        out_specs=out_specs,
        out_shape=out_shape,
        scratch_shapes=[pltpu.VMEM((256, width), F32), pltpu.VMEM((512, 256), F32)],
        compiler_params=pltpu.CompilerParams(vmem_limit_bytes=20 << 20),
        cost_estimate=pl.CostEstimate(
            flops=2 * 256 * 2048 * 3072 * info.shape[0], bytes_accessed=15_000_000, transcendentals=262144
        ),
    )(info, *operands)


def add_kernel(one, other, out):
    out[...] = (one[...] + other[...].astype(F32)).astype(BF16)


def add_rows(one, other):
    vmem = pl.BlockSpec(memory_space=pltpu.VMEM)
    return pl.pallas_call(
        add_kernel,
        in_specs=[vmem, vmem],
        out_specs=vmem,
        out_shape=pltpu.VMEM(one.shape, BF16),
        compiler_params=pltpu.CompilerParams(vmem_limit_bytes=2 << 20),
        cost_estimate=pl.CostEstimate(flops=300_000, bytes_accessed=2_000_000, transcendentals=0),
        name="add_rows",
    )(in_vmem(one), in_vmem(other))


def final_kernel(own, up_a, up_b, down_a, down_b, out):
    @pl.loop(0, 2)
    def _(group):
        for part, ups, downs in ((0, up_a, down_a), (128, up_b, down_b)):
            rows = pl.ds(pl.multiple_of(group * 64, 64), 64)
            at = pl.ds(pl.multiple_of(part + group * 64, 64), 64)
            out[at] = (own[at] + ups[rows].astype(F32) + downs[rows].astype(F32)).astype(BF16)


def final_sum(*operands):
    vmem = pl.BlockSpec(memory_space=pltpu.VMEM)
    return pl.pallas_call(
        final_kernel,
        in_specs=[vmem] * len(operands),
        out_specs=vmem,
        out_shape=jax.ShapeDtypeStruct(operands[0].shape, BF16),
        compiler_params=pltpu.CompilerParams(vmem_limit_bytes=8 << 20),
        cost_estimate=pl.CostEstimate(
            flops=2_000_000, bytes_accessed=5_000_000, transcendentals=0
        ),
        name="final",
    )(*(in_vmem(a) for a in operands))


def layer(
    residual, query, key, value, sink, norm_gain, w_out, w_gate, w_value, conv_gate, conv_value,
    w_down,
):
    count, width = residual.shape
    sp = lax.axis_index("sp")
    tp = lax.axis_index("tp")
    start = sp * count
    total = count * lax.axis_size("sp")
    core = sp % NC
    place_at = jnp.stack([sp // (NX * NC), (sp // NC) % NX, core]).astype(jnp.int32)

    gv_shard = jnp.concatenate([w_gate, w_value], axis=1)
    chunk, gv_1, late, gv_3 = gather_gv_rows(gv_shard, core)
    gv_2 = late
    chunk, key, value, query, residual_edge = lax.optimization_barrier(
        (chunk, key, value, query, (residual[:1], residual[count - 1:]))
    )
    down_pieces = gather_down(w_down.T, core, place_at, late)

    kv = jnp.concatenate([key, value], axis=1)

    def packed(rows, at, resid):
        return jnp.concatenate(
            [
                rows,
                query[at:at + 1].reshape(2, 128),
                resid.reshape(16, 128),
                jnp.zeros((14, 128), BF16),
            ],
            axis=0,
        )

    n_sp = lax.axis_size("sp")
    forward = [(i, i + 1) for i in range(n_sp - 1)]
    backward = [(i + 1, i) for i in range(n_sp - 1)]
    low = lax.ppermute(packed(kv[-HALO:], count - 1, residual_edge[1]), "sp", forward)
    high = lax.ppermute(packed(kv[:HALO], 0, residual_edge[0]), "sp", backward)
    low, high, _ = lax.optimization_barrier((low, high, late))
    kv_ext = jnp.concatenate([low[:HALO], kv, high[:HALO]], axis=0)

    def edges(width_128):
        at = HALO if width_128 == 2 else HALO + 2
        cols = width_128 * 128
        pad = jnp.zeros((EDGE - 1, cols), BF16)
        return jnp.concatenate(
            [
                pad,
                low[at:at + width_128].reshape(1, cols),
                high[at:at + width_128].reshape(1, cols),
                pad,
            ],
            axis=0,
        )

    q_edges = edges(2)
    res_edges = edges(16)

    wo_left = tp_shift(w_out)
    wo_mine = tp_shift(half_of(wo_left, core, 128))
    wo_right = sp_shift(wo_left, swap=True)
    wo_other = sp_shift(wo_mine, swap=True)

    rows_kv = count + 2 * HALO
    inverse = 1.0 / THETA ** (jnp.arange(0, HD, 2, dtype=F32) / HD)
    quarter_rows = rows_kv // 4
    lane = jnp.arange(128, dtype=jnp.int32)
    position = (
        (start - HALO)
        + jnp.arange(quarter_rows, dtype=jnp.int32)[:, None]
        + (lane // 32)[None, :] * quarter_rows
    ).astype(F32)
    angle = position * jnp.tile(inverse, 4)[None, :]

    start_ref = jnp.reshape(start, (1,)).astype(jnp.int32)
    mine = attention(start_ref, sink, query, q_edges, kv_ext, jnp.cos(angle), jnp.sin(angle), total)

    info = jnp.stack(
        [core, start, jnp.int32(total), tp, place_at[0], place_at[1]]
    ).astype(jnp.int32)
    pad8 = lambda taps: jnp.pad(taps.astype(F32), ((0, 5), (0, 0)))
    indices = tuple(
        jnp.stack([(tp + shift) % NY for shift in turns]).astype(jnp.int32)
        for turns in ((0,), (2,), (1, 3))
    )
    mine, info, place_late, taps, indices, res_edges, gain = lax.optimization_barrier(
        (mine, info, place_at, pad8(jnp.concatenate([conv_gate, conv_value], axis=1)), indices, res_edges,
         norm_gain.reshape(1, width))
    )

    gv_3, mine = lax.optimization_barrier((gv_3, mine))
    gv_mine, gv_theirs = gather_gv(gv_shard, core, gv_1, gv_2, gv_3)

    left = tp_shift(mine)
    right = tp_shift(mine, flip=-1)
    far_a = tp_shift(left[:512])
    far_b = tp_shift(right[512:], flip=-1)

    normed, mid, w_up = mix(
        info,
        (mine, left, right, far_a, far_b),
        (w_out, wo_left, wo_right, wo_mine, wo_other),
        residual,
        res_edges,
        gain,
        gv_mine[:1] + gv_theirs[:1],
        (width, 2 * w_gate.shape[1]),
    )

    w_dn = place(place_down_kernel, place_late, down_pieces, (width, w_gate.shape[1]), 9)
    sets = (gv_mine[1], gv_theirs[1], gv_mine[2], gv_theirs[2])
    w_up = place_rest(place_late, sets, (-1, 1), w_up)
    w_up = place_rest(place_late, (gv_mine[3], gv_theirs[3]), (-2,), w_up)

    def quarter(index, **kwargs):
        return ffn(index, normed, w_up, w_dn, taps, **kwargs)

    opp_a, opp_b = quarter(indices[1], dtypes=(BF16, BF16))
    from_low = tp_shift(opp_a, flip=1, by_core=False)
    from_high = tp_shift(opp_b, flip=-1, by_core=False)
    up_a, up_b, down_a, down_b = quarter(indices[2], dtypes=(F32, BF16, BF16, F32))
    got_up_b = tp_shift(up_b, flip=1, by_core=False)
    got_down_a = tp_shift(down_a, flip=-1, by_core=False)
    up_a = add_rows(up_a, from_low)
    got_up_a = tp_shift(up_a, flip=1, by_core=False)
    down_b = add_rows(down_b, from_high)
    got_down_b = tp_shift(down_b, flip=-1, by_core=False)
    own = quarter(indices[0], mid=mid)
    return final_sum(own, got_up_a, got_up_b, got_down_a, got_down_b)


def solution(mesh):
    return jax.shard_map(
        layer,
        mesh=mesh,
        in_specs=(
            P("sp", None),
            P("sp", "tp"),
            P("sp", "tp"),
            P("sp", "tp"),
            P("tp"),
            P(),
            P("tp", None),
            P("sp", "tp"),
            P("sp", "tp"),
            P(None, "tp"),
            P(None, "tp"),
            P("tp", "sp"),
        ),
        out_specs=P(("sp", "tp"), None),
        check_vma=False,
    )
```

```python
import functools

import jax
import jax.numpy as jnp
from jax import lax
from jax.experimental import pallas as pl
from jax.experimental.pallas import tpu as pltpu
from jax.sharding import PartitionSpec as P


HD = 64
WINDOW = 128
THETA = 10000.0
EPS = 1e-06
NZ, NX, NC, NY = 8, 4, 2, 4
EDGE = 16
HALO = WINDOW + EDGE
NEG = -1e30
F32 = jnp.float32
BF16 = jnp.bfloat16


def sp_index(z, x, c):
    return ((z % NZ) * NX + x % NX) * NC + c


def sp_shift(value, dz=0, dx=0, swap=False, flip=1):
    pairs = []
    for z in range(NZ):
        for x in range(NX):
            for c in range(NC):
                s = flip * (1 - 2 * c)
                target = sp_index(z, x, 1 - c) if swap else sp_index(z + s * dz, x + s * dx, c)
                pairs.append((sp_index(z, x, c), target))
    return lax.ppermute(value, "sp", pairs)


def tp_shift(value, flip=1, by_core=True):
    pairs = []
    for sp in range(NZ * NX * NC):
        s = flip * (1 - 2 * (sp % NC)) if by_core else flip
        for y in range(NY):
            pairs.append((sp * NY + y, sp * NY + (y + s) % NY))
    return lax.ppermute(value, ("sp", "tp"), pairs)


def in_vmem(value):
    return pltpu.with_memory_space_constraint(value, pltpu.VMEM)


def half_of(value, core, rows):
    return lax.dynamic_slice_in_dim(value, core * rows, rows, 0)


def joined(core, shard, sibling):
    return jnp.where(
        core == 0,
        jnp.concatenate([shard, sibling], 0),
        jnp.concatenate([sibling, shard], 0),
    )


def gather_gv_rows(shard, core):
    chunk = joined(core, shard, sp_shift(shard, swap=True))
    r1 = sp_shift(chunk, dz=1)
    r2 = sp_shift(r1, dz=1)
    r3 = sp_shift(r2, dz=1)
    return chunk, r1, r2, r3


def gather_gv(shard, core, r1, r2, r3):
    r4 = sp_shift(half_of(r3, core, 32), dz=1)
    h0 = jnp.concatenate([r1, r2, r3, r4, shard], 0)
    a1 = sp_shift(h0, dx=1)
    b1 = sp_shift(h0, dx=1, flip=-1)
    a2 = sp_shift(a1, dx=1)
    mine = (h0, a1, b1, a2)
    theirs = tuple(sp_shift(v, swap=True) for v in mine)
    return mine, theirs


def gather_down(shard, core, place_at, late, attended):
    chunk = joined(core, shard, sp_shift(shard, swap=True))
    r1 = sp_shift(chunk, dx=1)
    r1, _ = lax.optimization_barrier((r1, late))
    r2 = sp_shift(half_of(r1, core, 32), dx=1)
    r2, _ = lax.optimization_barrier((r2, attended))
    m = jnp.concatenate([shard, r1, r2], 0)
    other = sp_shift(m, swap=True)
    full = place(place_x_kernel, place_at, (m, other), (256, shard.shape[1]), 6)
    z1 = sp_shift(full, dz=1)
    z2 = sp_shift(z1, dz=1)
    z3 = sp_shift(z2, dz=1)
    half = place(place_half_kernel, place_at, (z3,), (128, shard.shape[1]), 1)
    z4 = sp_shift(half, dz=1)
    mine = (z1, z2, z3, z4)
    theirs = tuple(sp_shift(v, swap=True) for v in mine)
    return (full,) + mine + theirs


def copier(out, sems):
    copies = []

    def copy(src, at, rows, dst):
        copies.append(
            pltpu.make_async_copy(
                src.at[pl.ds(at, rows)],
                out.at[pl.ds(pl.multiple_of(dst, 32), rows)],
                sems.at[len(copies)],
            )
        )

    return copies, copy


def copies_of_set(copy, src, zxc, dx, other):
    z, x, c = zxc
    cc = 1 - c if other else c
    s = 1 - 2 * cc
    base = ((x + s * dx + NX) % NX) * 64
    for k in (1, 2, 3):
        copy(src, (k - 1) * 64, 64, ((z - s * k + NZ) % NZ) * 256 + base)
    copy(src, 192, 32, ((z + 4) % NZ) * 256 + base + cc * 32)
    copy(src, 224, 32, z * 256 + base + cc * 32)


def run_copies(copies):
    for item in copies:
        item.start()
    for item in copies:
        item.wait()


def place_rest_kernel(pos, *refs, offsets):
    count = 2 * len(offsets)
    pieces, out, sems = refs[:count], refs[count + 1], refs[count + 2]
    copies, copy = copier(out, sems)
    for index, dx in enumerate(offsets):
        for other in (False, True):
            src = pieces[2 * index + other]
            copies_of_set(copy, src, (pos[0], pos[1], pos[2]), dx, other)
    run_copies(copies)


def place_x_kernel(pos, mine, theirs, out, sems):
    x, c = pos[1], pos[2]
    copies, copy = copier(out, sems)
    for src, cc in ((mine, c), (theirs, 1 - c)):
        s = 1 - 2 * cc
        copy(src, 0, 32, x * 64 + cc * 32)
        copy(src, 32, 64, ((x - s + NX) % NX) * 64)
        copy(src, 96, 32, ((x + 2) % NX) * 64 + cc * 32)
    run_copies(copies)


def place_half_kernel(pos, src, out, sems):
    at = pl.multiple_of(pos[2] * 128, 128)
    copy = pltpu.make_async_copy(src.at[pl.ds(at, 128)], out, sems.at[0])
    copy.start()
    copy.wait()


def place_down_kernel(pos, *refs):
    pieces, out, sems = refs[:9], refs[9], refs[10]
    z, c = pos[0], pos[2]
    copies, copy = copier(out, sems)
    copy(pieces[0], 0, 256, z * 256)
    for side in range(2):
        cc = c if side == 0 else 1 - c
        s = 1 - 2 * cc
        for k in (1, 2, 3):
            copy(pieces[side * 4 + k], 0, 256, ((z - s * k + NZ) % NZ) * 256)
        copy(pieces[side * 4 + 4], 0, 128, ((z + 4) % NZ) * 256 + cc * 128)
    run_copies(copies)


def place_rest(pos, pieces, offsets, w_up):
    any_spec = pl.BlockSpec(memory_space=pl.ANY)
    vmem = pl.BlockSpec(memory_space=pltpu.VMEM)
    count = len(pieces)
    return pl.pallas_call(
        functools.partial(place_rest_kernel, offsets=offsets),
        in_specs=[pl.BlockSpec(memory_space=pltpu.SMEM)] + [any_spec] * count + [vmem],
        out_specs=vmem,
        out_shape=pltpu.VMEM(w_up.shape, BF16),
        input_output_aliases={count + 1: 0},
        scratch_shapes=[pltpu.SemaphoreType.DMA((5 * count,))],
        compiler_params=pltpu.CompilerParams(vmem_limit_bytes=2 << 20),
        cost_estimate=pl.CostEstimate(
            flops=20_000_000, bytes_accessed=2_000_000 * count, transcendentals=0
        ),
    )(pos, *pieces, in_vmem(w_up))


def place(kernel, pos, pieces, shape, count):
    any_spec = pl.BlockSpec(memory_space=pl.ANY)
    return pl.pallas_call(
        kernel,
        in_specs=[pl.BlockSpec(memory_space=pltpu.SMEM)] + [any_spec] * len(pieces),
        out_specs=pl.BlockSpec(memory_space=pltpu.VMEM),
        out_shape=pltpu.VMEM(shape, BF16),
        scratch_shapes=[pltpu.SemaphoreType.DMA((count,))],
        compiler_params=pltpu.CompilerParams(vmem_limit_bytes=2 << 20),
        cost_estimate=pl.CostEstimate(
            flops=20_000_000, bytes_accessed=4 * shape[0] * shape[1], transcendentals=0
        ),
    )(pos, *pieces)


def attention_kernel(start_ref, sink_ref, q_ref, edge_ref, kv_ref, cos_ref, sin_ref, out_ref,
                     cos_s, sin_s, kr_s, vx_s, *, total):
    step = pl.program_id(0)
    start = start_ref[0]
    rows_kv = kv_ref.shape[0]
    packed = rows_kv // 4

    @pl.when(step == 0)
    def _():
        lane_p = lax.broadcasted_iota(jnp.int32, (packed, 128), 1)

        def spread(table, part):
            one = jnp.where(lane_p // 32 == part, table, 0.0)
            one = one + pltpu.roll(one, 32, 1)
            return one + pltpu.roll(one, 64, 1)

        sign = jnp.where(lane_p % 64 < 32, -1.0, 1.0)
        cos_p, sin_p = cos_ref[...], sin_ref[...]
        for part in range(4):
            cos_s[part * packed:(part + 1) * packed] = spread(cos_p, part)
            sin_s[part * packed:(part + 1) * packed] = spread(sin_p, part) * sign
        kv = kv_ref[...].astype(F32)
        lane = lax.broadcasted_iota(jnp.int32, (rows_kv, 128), 1)
        swapped = jnp.where(lane % 64 < 32, pltpu.roll(kv, 96, 1), pltpu.roll(kv, 32, 1))
        turned = kv * cos_s[...] + swapped * sin_s[...]
        kr_s[...] = jnp.where(lane < 64, turned, 0.0).astype(BF16)
        vx_s[...] = jnp.where(lane < 64, pltpu.roll(kv, 64, 1), 1.0).astype(BF16)

    def attend(q, at, window, first, out_at):
        rows = q.shape[0]
        span = 3 * WINDOW
        lane = lax.broadcasted_iota(jnp.int32, (rows, 128), 1)
        cos = cos_s[pl.ds(at, rows)]
        sin = sin_s[pl.ds(at, rows)]
        stack = []
        for pair in range(2):
            part = q[:, pair * 128:(pair + 1) * 128].astype(F32)
            swapped = jnp.where(lane % 64 < 32, pltpu.roll(part, 96, 1), pltpu.roll(part, 32, 1))
            turned = (part * cos + swapped * sin).astype(BF16).astype(F32) * HD ** (-0.5)
            stack.append(jnp.where(lane < 64, turned, 0.0).astype(BF16))
            stack.append(jnp.where(lane < 64, pltpu.roll(turned, 64, 1), 0.0).astype(BF16))
        stacked = jnp.concatenate(stack, axis=0)
        keys = kr_s[pl.ds(window, span)]
        values = vx_s[pl.ds(window, span)]
        scores = lax.dot_general(
            stacked, keys, (((1,), (1,)), ((), ())), preferred_element_type=F32
        )
        row_pos = first + lax.broadcasted_iota(jnp.int32, (rows, span), 0)
        col_pos = (start - HALO + window) + lax.broadcasted_iota(jnp.int32, (rows, span), 1)
        apart = row_pos - col_pos
        valid = (apart <= WINDOW) & (apart >= -WINDOW) & (col_pos >= 0) & (col_pos < total)
        weights, sink_terms = [], []
        for head in range(4):
            mine = jnp.where(valid, scores[head * rows:(head + 1) * rows], NEG)
            sink = sink_ref[head]
            top = jnp.maximum(jnp.max(mine, axis=1, keepdims=True), sink)
            weights.append(jnp.exp(mine - top).astype(BF16))
            sink_terms.append(jnp.exp(sink - top))
        both = jnp.dot(jnp.concatenate(weights, axis=0), values, preferred_element_type=F32)
        heads = []
        for head in range(4):
            mine = both[head * rows:(head + 1) * rows]
            heads.append(mine / (pltpu.roll(mine, 64, 1) + sink_terms[head]))
        for pair in range(2):
            joined = jnp.where(lane < 64, heads[2 * pair], pltpu.roll(heads[2 * pair + 1], 64, 1))
            out_ref[pl.ds(out_at, rows), pair * 128:(pair + 1) * 128] = joined.astype(BF16)

    base = pl.multiple_of(step * WINDOW, WINDOW)
    attend(q_ref[...], base + HALO, base + EDGE, start + base, base)

    @pl.when(step == pl.num_programs(0) - 1)
    def _():
        count = out_ref.shape[0] - 2 * EDGE

        @pl.loop(0, 2)
        def _(side):
            at = pl.multiple_of(side * EDGE, EDGE)
            attend(
                edge_ref[pl.ds(at, EDGE)],
                pl.multiple_of(HALO - EDGE + side * (count + EDGE), EDGE),
                pl.multiple_of(side * (rows_kv - 3 * WINDOW), EDGE),
                start - EDGE + side * (count + EDGE),
                pl.multiple_of(count + at, EDGE),
            )


def attention(start, sink, query, edges, kv, cos, sin, total):
    count = query.shape[0]
    rows_kv = kv.shape[0]
    blocks = count // WINDOW
    whole = lambda shape: pl.BlockSpec(shape, lambda i: (0, 0))
    smem = pl.BlockSpec(memory_space=pltpu.SMEM)
    return pl.pallas_call(
        functools.partial(attention_kernel, total=total),
        grid=(blocks,),
        in_specs=[
            smem,
            smem,
            pl.BlockSpec((WINDOW, 256), lambda i: (i, 0)),
            whole(edges.shape),
            whole(kv.shape),
            whole(cos.shape),
            whole(sin.shape),
        ],
        out_specs=whole((count + 2 * EDGE, 256)),
        out_shape=jax.ShapeDtypeStruct((count + 2 * EDGE, 256), BF16),
        scratch_shapes=[
            pltpu.VMEM((rows_kv, 128), F32),
            pltpu.VMEM((rows_kv, 128), F32),
            pltpu.VMEM((rows_kv, 128), BF16),
            pltpu.VMEM((rows_kv, 128), BF16),
        ],
        compiler_params=pltpu.CompilerParams(
            dimension_semantics=("arbitrary",), vmem_limit_bytes=16 << 20
        ),
        cost_estimate=pl.CostEstimate(
            flops=1_600_000_000, bytes_accessed=3_000_000, transcendentals=1_700_000
        ),
        name="attention",
    )(start, sink, query, edges, kv, cos, sin)


def mix_kernel(info, own, left, right, far_a, far_b, w_own, w_left, w_right, w_mine, w_other,
               res, res_edge, gain, h0, h0t, norm_ref, mid_ref, up_ref,
               far, w_far, acc, sems):
    core, start, total, tp = info[0], info[1], info[2], info[3]
    zxc = (info[4], info[5], core)
    copies, copy = copier(up_ref, sems)
    copies_of_set(copy, h0, zxc, 0, False)
    copies_of_set(copy, h0t, zxc, 0, True)
    for item in copies:
        item.start()
    count = res.shape[0]
    far[:far_a.shape[0]] = far_a[...]
    far[far_a.shape[0]:] = far_b[...]
    w_far[pl.ds(pl.multiple_of(core * 128, 128), 128)] = w_mine[...]
    w_far[pl.ds(pl.multiple_of((1 - core) * 128, 128), 128)] = w_other[...]

    width = res.shape[1]
    step = 512

    def project(at, rows, resid, out):
        @pl.loop(0, width // step)
        def _(index):
            cols = pl.ds(pl.multiple_of(index * step, step), step)
            term = resid(cols).astype(F32)
            for ref, weight in ((own, w_own), (left, w_left), (right, w_right), (far, w_far)):
                term = term + jnp.dot(
                    ref[pl.ds(at, rows)], weight[:, cols], preferred_element_type=F32
                )
            out[:rows, cols] = term

    def norm(total):
        mid = total.astype(BF16)
        wide = mid.astype(F32)
        scale = lax.rsqrt(jnp.mean(wide * wide, axis=1, keepdims=True) + EPS)
        return mid, wide * scale * gain[...]

    @pl.loop(0, count // 256)
    def _(part):
        at = pl.multiple_of(part * 256, 256)
        project(at, 256, lambda cols: res[pl.ds(at, 256), cols], acc)

        @pl.loop(0, 4)
        def _(group):
            rows = pl.multiple_of(group * 64, 64)
            mid, normed = norm(acc[pl.ds(rows, 64)])
            norm_ref[pl.ds(pl.multiple_of(EDGE + at + rows, EDGE), 64)] = normed.astype(BF16)

            @pl.when(tp == part)
            def _():
                mid_ref[pl.ds(rows, 64)] = mid

    project(count, 2 * EDGE, lambda cols: res_edge[:, cols], acc)
    _, normed = norm(acc[:2 * EDGE])
    index = lax.broadcasted_iota(jnp.int32, (2 * EDGE, 1), 0)
    pos = start - EDGE + index + jnp.where(index < EDGE, 0, count)
    inside = (pos >= 0) & (pos < total)
    normed = jnp.where(inside, normed, 0.0).astype(BF16)
    norm_ref[0:EDGE] = normed[:EDGE]
    norm_ref[EDGE + count:2 * EDGE + count] = normed[EDGE:]
    for item in copies:
        item.wait()


def mix(info, parts, weights, residual, res_edges, gain, pieces, up_shape):
    count, width = residual.shape
    vmem = pl.BlockSpec(memory_space=pltpu.VMEM)
    any_spec = pl.BlockSpec(memory_space=pl.ANY)
    operands = [in_vmem(a) for a in (*parts, *weights, residual)] + [res_edges, gain]
    return pl.pallas_call(
        mix_kernel,
        in_specs=[pl.BlockSpec(memory_space=pltpu.SMEM)] + [vmem] * len(operands)
        + [any_spec] * len(pieces),
        out_specs=[vmem, vmem, vmem],
        out_shape=[
            pltpu.VMEM((count + 2 * EDGE, width), BF16),
            pltpu.VMEM((256, width), BF16),
            pltpu.VMEM(up_shape, BF16),
        ],
        scratch_shapes=[
            pltpu.VMEM((count + 2 * EDGE, 256), BF16),
            pltpu.VMEM((256, width), BF16),
            pltpu.VMEM((256, width), F32),
            pltpu.SemaphoreType.DMA((10,)),
        ],
        compiler_params=pltpu.CompilerParams(vmem_limit_bytes=20 << 20),
        cost_estimate=pl.CostEstimate(
            flops=2 * 1056 * 1024 * 2048, bytes_accessed=20_000_000, transcendentals=1056
        ),
        name="mix",
    )(info, *operands, *pieces)


def ffn_kernel(info, x, w_up, w_dn, taps_all, *rest):
    rest, acc, conv = rest[:-2], rest[-2], rest[-1]
    rows = 256 + 2 * EDGE
    hidden_all = w_dn.shape[1]
    block = 256

    @pl.loop(0, info.shape[0])
    def _(turn):
        at = pl.multiple_of(info[turn] * 256, 256)

        def convolve(first, taps):
            up = jnp.dot(
                x[pl.ds(at, rows)], w_up[:, pl.ds(first, block)], preferred_element_type=F32
            )
            up = up.astype(BF16).astype(F32)
            out = (
                pltpu.roll(up, 1, 0) * taps[0:1]
                + up * taps[1:2]
                + pltpu.roll(up, rows - 1, 0) * taps[2:3]
            )
            return out[EDGE:EDGE + 256]

        if rest[0].shape[0] == 256:
            acc[...] = rest[0][...].astype(F32)
        else:
            acc[...] = jnp.zeros(acc.shape, F32)

        @pl.loop(0, hidden_all // block)
        def _(step):
            first = pl.multiple_of(step * block, block)

            @pl.loop(0, 2)
            def _(side):
                cols = pl.multiple_of(side * hidden_all + first, block)
                conv[pl.ds(pl.multiple_of(side * 256, 256), 256)] = convolve(
                    cols, taps_all[:, pl.ds(cols, block)]
                )

            gate, value = conv[:256], conv[256:]
            hidden = (gate / (1.0 + jnp.exp(-gate)) * value).astype(BF16)
            acc[...] += lax.dot_general(
                hidden, w_dn[:, pl.ds(first, block)], (((1,), (1,)), ((), ())),
                preferred_element_type=F32,
            )

        outs = rest[-1:] if rest[-1].shape[0] == 256 else rest
        for index in range(len(outs) // 2):
            @pl.when(turn == index)
            def _():
                outs[2 * index][...] = acc[:128].astype(outs[2 * index].dtype)
                outs[2 * index + 1][...] = acc[128:].astype(outs[2 * index + 1].dtype)
        if len(outs) == 1:
            outs[0][...] = acc[...]


def ffn(info, normed, w_up, w_down, taps, dtypes=None, mid=None):
    width = normed.shape[1]
    vmem = pl.BlockSpec(memory_space=pltpu.VMEM)
    operands = [in_vmem(normed), in_vmem(w_up), in_vmem(w_down), taps]
    if mid is None:
        out_shape = [pltpu.VMEM((128, width), d) for d in dtypes]
        out_specs = [vmem] * len(dtypes)
    else:
        operands.append(in_vmem(mid))
        out_shape, out_specs = pltpu.VMEM((256, width), F32), vmem
    return pl.pallas_call(
        ffn_kernel,
        in_specs=[pl.BlockSpec(memory_space=pltpu.SMEM)] + [vmem] * len(operands),
        out_specs=out_specs,
        out_shape=out_shape,
        scratch_shapes=[pltpu.VMEM((256, width), F32), pltpu.VMEM((512, 256), F32)],
        compiler_params=pltpu.CompilerParams(vmem_limit_bytes=20 << 20),
        cost_estimate=pl.CostEstimate(
            flops=2 * 256 * 2048 * 3072 * info.shape[0], bytes_accessed=15_000_000, transcendentals=262144
        ),
    )(info, *operands)


def add_kernel(one, other, out):
    out[...] = (one[...] + other[...].astype(F32)).astype(BF16)


def add_rows(one, other):
    vmem = pl.BlockSpec(memory_space=pltpu.VMEM)
    return pl.pallas_call(
        add_kernel,
        in_specs=[vmem, vmem],
        out_specs=vmem,
        out_shape=pltpu.VMEM(one.shape, BF16),
        compiler_params=pltpu.CompilerParams(vmem_limit_bytes=2 << 20),
        cost_estimate=pl.CostEstimate(flops=300_000, bytes_accessed=2_000_000, transcendentals=0),
        name="add_rows",
    )(in_vmem(one), in_vmem(other))


def final_kernel(own, up_a, up_b, down_a, down_b, out):
    @pl.loop(0, 2)
    def _(group):
        for part, ups, downs in ((0, up_a, down_a), (128, up_b, down_b)):
            rows = pl.ds(pl.multiple_of(group * 64, 64), 64)
            at = pl.ds(pl.multiple_of(part + group * 64, 64), 64)
            out[at] = (own[at] + ups[rows].astype(F32) + downs[rows].astype(F32)).astype(BF16)


def final_sum(*operands):
    vmem = pl.BlockSpec(memory_space=pltpu.VMEM)
    return pl.pallas_call(
        final_kernel,
        in_specs=[vmem] * len(operands),
        out_specs=vmem,
        out_shape=jax.ShapeDtypeStruct(operands[0].shape, BF16),
        compiler_params=pltpu.CompilerParams(vmem_limit_bytes=8 << 20),
        cost_estimate=pl.CostEstimate(
            flops=2_000_000, bytes_accessed=5_000_000, transcendentals=0
        ),
        name="final",
    )(*(in_vmem(a) for a in operands))


def layer(
    residual, query, key, value, sink, norm_gain, w_out, w_gate, w_value, conv_gate, conv_value,
    w_down,
):
    count, width = residual.shape
    sp = lax.axis_index("sp")
    tp = lax.axis_index("tp")
    start = sp * count
    total = count * lax.axis_size("sp")
    core = sp % NC
    place_at = jnp.stack([sp // (NX * NC), (sp // NC) % NX, core]).astype(jnp.int32)

    gv_shard = jnp.concatenate([w_gate, w_value], axis=1)
    chunk, gv_1, late, gv_3 = gather_gv_rows(gv_shard, core)
    gv_2 = late
    chunk, key, value, query, residual_edge = lax.optimization_barrier(
        (chunk, key, value, query, (residual[:1], residual[count - 1:]))
    )

    kv = jnp.concatenate([key, value], axis=1)

    def packed(rows, at, resid):
        return jnp.concatenate(
            [
                rows,
                query[at:at + 1].reshape(2, 128),
                resid.reshape(16, 128),
                jnp.zeros((14, 128), BF16),
            ],
            axis=0,
        )

    n_sp = lax.axis_size("sp")
    forward = [(i, i + 1) for i in range(n_sp - 1)]
    backward = [(i + 1, i) for i in range(n_sp - 1)]
    low = lax.ppermute(packed(kv[-HALO:], count - 1, residual_edge[1]), "sp", forward)
    high = lax.ppermute(packed(kv[:HALO], 0, residual_edge[0]), "sp", backward)
    low, high, _ = lax.optimization_barrier((low, high, late))
    kv_ext = jnp.concatenate([low[:HALO], kv, high[:HALO]], axis=0)

    def edges(width_128):
        at = HALO if width_128 == 2 else HALO + 2
        cols = width_128 * 128
        pad = jnp.zeros((EDGE - 1, cols), BF16)
        return jnp.concatenate(
            [
                pad,
                low[at:at + width_128].reshape(1, cols),
                high[at:at + width_128].reshape(1, cols),
                pad,
            ],
            axis=0,
        )

    q_edges = edges(2)
    res_edges = edges(16)

    wo_left = tp_shift(w_out)
    wo_mine = tp_shift(half_of(wo_left, core, 128))
    wo_right = sp_shift(wo_left, swap=True)
    wo_other = sp_shift(wo_mine, swap=True)

    rows_kv = count + 2 * HALO
    inverse = 1.0 / THETA ** (jnp.arange(0, HD, 2, dtype=F32) / HD)
    quarter_rows = rows_kv // 4
    lane = jnp.arange(128, dtype=jnp.int32)
    position = (
        (start - HALO)
        + jnp.arange(quarter_rows, dtype=jnp.int32)[:, None]
        + (lane // 32)[None, :] * quarter_rows
    ).astype(F32)
    angle = position * jnp.tile(inverse, 4)[None, :]

    start_ref = jnp.reshape(start, (1,)).astype(jnp.int32)
    mine = attention(start_ref, sink, query, q_edges, kv_ext, jnp.cos(angle), jnp.sin(angle), total)

    down_pieces = gather_down(w_down.T, core, place_at, late, mine)

    info = jnp.stack(
        [core, start, jnp.int32(total), tp, place_at[0], place_at[1]]
    ).astype(jnp.int32)
    pad8 = lambda taps: jnp.pad(taps.astype(F32), ((0, 5), (0, 0)))
    indices = tuple(
        jnp.stack([(tp + shift) % NY for shift in turns]).astype(jnp.int32)
        for turns in ((0,), (2,), (1, 3))
    )
    mine, info, place_late, taps, indices, res_edges, gain = lax.optimization_barrier(
        (mine, info, place_at, pad8(jnp.concatenate([conv_gate, conv_value], axis=1)), indices, res_edges,
         norm_gain.reshape(1, width))
    )

    gv_3, mine = lax.optimization_barrier((gv_3, mine))
    gv_mine, gv_theirs = gather_gv(gv_shard, core, gv_1, gv_2, gv_3)

    left = tp_shift(mine)
    right = tp_shift(mine, flip=-1)
    far_a = tp_shift(left[:512])
    far_b = tp_shift(right[512:], flip=-1)

    normed, mid, w_up = mix(
        info,
        (mine, left, right, far_a, far_b),
        (w_out, wo_left, wo_right, wo_mine, wo_other),
        residual,
        res_edges,
        gain,
        gv_mine[:1] + gv_theirs[:1],
        (width, 2 * w_gate.shape[1]),
    )

    w_dn = place(place_down_kernel, place_late, down_pieces, (width, w_gate.shape[1]), 9)
    sets = (gv_mine[1], gv_theirs[1], gv_mine[2], gv_theirs[2])
    w_up = place_rest(place_late, sets, (-1, 1), w_up)
    w_up = place_rest(place_late, (gv_mine[3], gv_theirs[3]), (-2,), w_up)

    def quarter(index, **kwargs):
        return ffn(index, normed, w_up, w_dn, taps, **kwargs)

    opp_a, opp_b = quarter(indices[1], dtypes=(BF16, BF16))
    from_low = tp_shift(opp_a, flip=1, by_core=False)
    from_high = tp_shift(opp_b, flip=-1, by_core=False)
    up_a, up_b, down_a, down_b = quarter(indices[2], dtypes=(F32, BF16, BF16, F32))
    got_up_b = tp_shift(up_b, flip=1, by_core=False)
    got_down_a = tp_shift(down_a, flip=-1, by_core=False)
    up_a = add_rows(up_a, from_low)
    got_up_a = tp_shift(up_a, flip=1, by_core=False)
    down_b = add_rows(down_b, from_high)
    got_down_b = tp_shift(down_b, flip=-1, by_core=False)
    own = quarter(indices[0], mid=mid)
    return final_sum(own, got_up_a, got_up_b, got_down_a, got_down_b)


def solution(mesh):
    return jax.shard_map(
        layer,
        mesh=mesh,
        in_specs=(
            P("sp", None),
            P("sp", "tp"),
            P("sp", "tp"),
            P("sp", "tp"),
            P("tp"),
            P(),
            P("tp", None),
            P("sp", "tp"),
            P("sp", "tp"),
            P(None, "tp"),
            P(None, "tp"),
            P("tp", "sp"),
        ),
        out_specs=P(("sp", "tp"), None),
        check_vma=False,
    )
```
